32 devices in a mesh: sp: 8 (over z, y), tp: 4 (over x, core).
Axes of the slice: x: 2, y: 2, z: 4, core: 2. Of those that a mesh axis runs over, the one named last changes fastest.
Arguments:
- tokens: bfloat16 [2048, 2048], P('sp'), may hold values from -72 to 72
- query_weight: bfloat16 [3, 2048, 1024], P(None, None, 'tp'), may hold values from -0.125 to 0.125
- key_weight: bfloat16 [3, 2048, 1024], P(None, None, 'tp'), may hold values from -0.125 to 0.125
- value_weight: bfloat16 [3, 2048, 1024], P(None, None, 'tp'), may hold values from -0.125 to 0.125
- out_weight: bfloat16 [1024, 2048], P(None, 'tp'), may hold values from -2 to 2
Outputs:
- mixed: bfloat16 [2048, 2048], P('sp', 'tp')
The draws below stay inside these ranges and needn't reach their ends.
All inputs are finite; a program needn't handle non-finite values.
Results may differ from the reference program's by a relative error of at most 0.012.
Values may be sent and summed in bfloat16 or wider, within the bound.
A program may use at most 64 MiB of HBM per device.

```python
import math
import jax
import jax.numpy as jnp
from jax import lax

D = 2048
SLOTS = 16
HEAD_DIM = 64
SIDE_STEPS = 64
MIDDLE_DILATION = 4
FAR_DILATION = 16
HW = 1024
TOKENS = 2048


def draw_tokens(key, part):
    base = jnp.clip(jax.random.normal(key, (TOKENS, D), jnp.float32), -6.0, 6.0)
    return base.astype(jnp.bfloat16)


def shard_levels(stream_key, extent, cuts, low, high):
    def one(position, blocks):
        draws = jax.random.uniform(jax.random.fold_in(jax.random.fold_in(stream_key, 6), position), (blocks,), jnp.float32, low / len(cuts), high / len(cuts))
        return jnp.repeat(jnp.exp(draws), extent[position] // blocks).reshape((-1,) + (1,) * (len(extent) - position - 1))

    level = one(*cuts[0])
    for cut in cuts[1:]:
        level = level * one(*cut)
    return level


def centred(rng, shape, spread, limit, pieces=(), kind=jnp.bfloat16):
    values = jax.random.normal(rng, shape, jnp.float32) * spread
    if len(pieces) > 0:
        values = shard_levels(rng, shape, pieces, -0.22, 0.18) * values
    return jnp.clip(values, min=-limit, max=limit).astype(kind)


def setup_inputs(seed: int = 0) -> dict:
    seeds = jax.random.split(jax.random.key(seed), 6)
    return {
        "tokens": draw_tokens(jax.random.fold_in(seeds[5], 71), 0),
        "query_weight": centred(seeds[1], (3, D, HW), D ** -0.5, 0.125, ((2, 4),)),
        "key_weight": centred(seeds[2], (3, D, HW), D ** -0.5, 0.125, ((2, 4),)),
        "value_weight": centred(seeds[3], (3, D, HW), D ** -0.5, 0.125, ((2, 4),)),
        "out_weight": centred(seeds[4], (HW, D), (HW // 128) ** -0.5, 2.0, ((1, 4),)),
    }


def rotate(projected, offset_pos):
    length, columns = projected.shape
    heads = columns // HEAD_DIM
    half = HEAD_DIM // 2
    positions = (offset_pos + jnp.arange(length)).astype(jnp.float32)
    inverse = 1.0 / (10000.0 ** (jnp.arange(half, dtype=jnp.float32) * 2.0 / HEAD_DIM))
    angles = positions[:, None] * inverse[None, :]
    angles = jnp.concatenate([angles, angles], axis=-1)
    cosine_table = jnp.cos(angles)[:, None, :]
    sine = jnp.sin(angles)[:, None, :]
    shaped = projected.reshape(length, heads, HEAD_DIM)
    turned = jnp.concatenate([-shaped[..., half:], shaped[..., :half]], axis=-1)
    return (shaped * cosine_table + turned * sine).reshape(length, columns)


def banded(queries, key_ext, value_ext, dilation, offset_pos, seq_len):
    length, columns = queries.shape
    heads = columns // HEAD_DIM
    class_len = length // dilation
    block_len = math.gcd(SIDE_STEPS, class_len)
    blocks = class_len // block_len
    extra = 2 * SIDE_STEPS // block_len
    query_blocks = queries.reshape(blocks, block_len, dilation, heads, HEAD_DIM)
    key_blocks = key_ext.reshape(blocks + extra, block_len, dilation, heads, HEAD_DIM)
    value_blocks = value_ext.reshape(blocks + extra, block_len, dilation, heads, HEAD_DIM)
    key_win = jnp.concatenate([key_blocks[shift_idx:shift_idx + blocks] for shift_idx in range(extra + 1)], axis=1)
    value_win = jnp.concatenate([value_blocks[shift_idx:shift_idx + blocks] for shift_idx in range(extra + 1)], axis=1)
    scores = jnp.einsum('bqrhe,bkrhe->brhqk', query_blocks.astype(jnp.float32), key_win.astype(jnp.float32))
    scores = scores * (HEAD_DIM ** -0.5)
    width_keys = key_win.shape[1]
    relative = jnp.arange(width_keys)[None, :] - jnp.arange(block_len)[:, None]
    within = (relative >= 0) & (relative <= 2 * SIDE_STEPS)
    key_rows = jnp.arange(blocks)[:, None] * block_len + jnp.arange(width_keys)[None, :]
    spots = offset_pos - SIDE_STEPS * dilation + dilation * key_rows[:, :, None] + jnp.arange(dilation)[None, None, :]
    inside = (spots >= 0) & (spots < seq_len)
    allowed = within[None, None, None] & jnp.transpose(inside, (0, 2, 1))[:, :, None, None, :]
    scores = jnp.where(allowed, scores, -1e30)
    row_max = jnp.max(scores, axis=-1, keepdims=True)
    expo = jnp.exp(scores - row_max)
    denom = jnp.sum(expo, axis=-1)
    probs = lax.optimization_barrier(expo.astype(jnp.bfloat16))
    summed = jnp.einsum('brhqk,bkrhe->bqrhe', probs.astype(jnp.float32), value_win.astype(jnp.float32))
    group_out = summed / jnp.transpose(denom, (0, 3, 1, 2))[..., None]
    log_sum = row_max[..., 0] + jnp.log(denom)
    log_sum = jnp.transpose(log_sum, (0, 3, 1, 2)).reshape(length, heads)
    return group_out.reshape(length, columns), log_sum


def reference(tokens, query_weight, key_weight, value_weight, out_weight):
    seq_len = tokens.shape[0]
    group_dilations = (1, MIDDLE_DILATION, FAR_DILATION)
    outputs = []
    log_sums = []
    for group_idx in range(3):
        queries = rotate(jnp.dot(tokens, query_weight[group_idx], preferred_element_type=jnp.float32), 0).astype(jnp.bfloat16)
        keys_all = rotate(jnp.dot(tokens, key_weight[group_idx], preferred_element_type=jnp.float32), 0).astype(jnp.bfloat16)
        value_rows_full = jnp.dot(tokens, value_weight[group_idx], preferred_element_type=jnp.float32).astype(jnp.bfloat16)
        reach = SIDE_STEPS * group_dilations[group_idx]
        key_ext = jnp.pad(keys_all, ((reach, reach), (0, 0)))
        value_ext = jnp.pad(value_rows_full, ((reach, reach), (0, 0)))
        group_out, log_sum = banded(queries, key_ext, value_ext, group_dilations[group_idx], 0, seq_len)
        outputs.append(group_out)
        log_sums.append(log_sum)
    merge_w = jax.nn.softmax(jnp.stack(log_sums, axis=0), axis=0)
    stacked = jnp.stack(outputs, axis=0).reshape(3, seq_len, SLOTS, HEAD_DIM)
    merged = jnp.sum(merge_w[..., None] * stacked, axis=0).reshape(seq_len, HW).astype(jnp.bfloat16)
    return jnp.dot(merged, out_weight, preferred_element_type=jnp.float32).astype(jnp.bfloat16)
```

```python
import functools
import math

import jax
import numpy as np
import jax.numpy as jnp
from jax import lax
from jax.experimental import pallas as pl
from jax.experimental.pallas import tpu as pltpu
from jax.sharding import PartitionSpec as P

HEAD_DIM = 64
SIDE_STEPS = 64
MIDDLE_DILATION = 4
FAR_DILATION = 16
MESH = pl.DeviceIdType.MESH


def shifted(block, axis, distance):
    devices = range(lax.axis_size(axis))
    route = [(i - distance, i) for i in devices if i - distance in devices]
    return lax.ppermute(block, axis, route)


def with_halo(block, sides, width):
    for axis, dim in sides:
        count = lax.axis_size(axis)
        forward = [(i, i + 1) for i in range(count - 1)]
        backward = [(target, source) for source, target in forward]
        low = lax.ppermute(
            lax.slice_in_dim(block, block.shape[dim] - width, None, axis=dim), axis, forward
        )
        high = lax.ppermute(lax.slice_in_dim(block, 0, width, axis=dim), axis, backward)
        block = jnp.concatenate([low, block, high], axis=dim)
    return block


def rotate(projected, offset_pos):
    length, columns = projected.shape
    heads = columns // HEAD_DIM
    half = HEAD_DIM // 2
    positions = (offset_pos + jnp.arange(length)).astype(jnp.float32)
    inverse = 1.0 / 10000.0 ** (jnp.arange(half, dtype=jnp.float32) * 2.0 / HEAD_DIM)
    angles = positions[:, None] * inverse[None, :]
    angles = jnp.concatenate([angles, angles], axis=-1)
    cosine_table = jnp.cos(angles)[:, None, :]
    sine = jnp.sin(angles)[:, None, :]
    shaped = projected.reshape(length, heads, HEAD_DIM)
    turned = jnp.concatenate([-shaped[..., half:], shaped[..., :half]], axis=-1)
    return (shaped * cosine_table + turned * sine).reshape(length, columns)


def banded(queries, key_ext, value_ext, dilation, offset_pos, seq_len):
    length, columns = queries.shape
    heads = columns // HEAD_DIM
    class_len = length // dilation
    block_len = math.gcd(SIDE_STEPS, class_len)
    blocks = class_len // block_len
    extra = 2 * SIDE_STEPS // block_len
    query_blocks = queries.reshape(blocks, block_len, dilation, heads, HEAD_DIM)
    key_blocks = key_ext.reshape(blocks + extra, block_len, dilation, heads, HEAD_DIM)
    value_blocks = value_ext.reshape(blocks + extra, block_len, dilation, heads, HEAD_DIM)
    key_win = jnp.concatenate(
        [key_blocks[shift_idx : shift_idx + blocks] for shift_idx in range(extra + 1)], axis=1
    )
    value_win = jnp.concatenate(
        [value_blocks[shift_idx : shift_idx + blocks] for shift_idx in range(extra + 1)], axis=1
    )
    scores = jnp.einsum(
        "bqrhe,bkrhe->brhqk", query_blocks, key_win, preferred_element_type=jnp.float32
    )
    scores = scores * HEAD_DIM ** (-0.5)
    width_keys = key_win.shape[1]
    relative = jnp.arange(width_keys)[None, :] - jnp.arange(block_len)[:, None]
    within = (relative >= 0) & (relative <= 2 * SIDE_STEPS)
    key_rows = jnp.arange(blocks)[:, None] * block_len + jnp.arange(width_keys)[None, :]
    spots = (
        offset_pos
        - SIDE_STEPS * dilation
        + dilation * key_rows[:, :, None]
        + jnp.arange(dilation)[None, None, :]
    )
    inside = (spots >= 0) & (spots < seq_len)
    allowed = within[None, None, None] & jnp.transpose(inside, (0, 2, 1))[:, :, None, None, :]
    scores = jnp.where(allowed, scores, -1e30)
    row_max = jnp.max(scores, axis=-1, keepdims=True)
    expo = jnp.exp(scores - row_max)
    denom = jnp.sum(expo, axis=-1)
    probs = expo.astype(jnp.bfloat16)
    summed = jnp.einsum("brhqk,bkrhe->bqrhe", probs, value_win, preferred_element_type=jnp.float32)
    group_out = summed / jnp.transpose(denom, (0, 3, 1, 2))[..., None]
    log_sum = row_max[..., 0] + jnp.log(denom)
    log_sum = jnp.transpose(log_sum, (0, 3, 1, 2)).reshape(length, heads)
    return (group_out.reshape(length, columns), log_sum)


def collect(own_block, needed, direction):
    collected = own_block[None]
    while collected.shape[0] < needed + 1:
        stride = collected.shape[0]
        to_send = min(stride, needed + 1 - stride)
        arrived = shifted(collected[:to_send], "sp", direction * stride)
        collected = jnp.concatenate([collected, arrived], axis=0)
    return collected[1:]


def per_device(tokens, query_weight, key_weight, value_weight, out_weight):
    length = tokens.shape[0]
    offset_pos = lax.axis_index("sp") * length
    seq_len = lax.axis_size("sp") * length
    group_dilations = (1, MIDDLE_DILATION, FAR_DILATION)
    query_list = []
    pairs = []
    for group_idx in range(3):
        queries = rotate(
            jnp.dot(tokens, query_weight[group_idx], preferred_element_type=jnp.float32), offset_pos
        )
        keys_here = rotate(
            jnp.dot(tokens, key_weight[group_idx], preferred_element_type=jnp.float32), offset_pos
        )
        values_here = jnp.dot(tokens, value_weight[group_idx], preferred_element_type=jnp.float32)
        query_list.append(queries.astype(jnp.bfloat16))
        pairs.append(
            jnp.stack([keys_here.astype(jnp.bfloat16), values_here.astype(jnp.bfloat16)], axis=0)
        )
    middle_span_length = SIDE_STEPS * MIDDLE_DILATION
    first_ext = with_halo(pairs[0], (("sp", 1),), SIDE_STEPS)
    middle_ext = with_halo(pairs[1], (("sp", 1),), middle_span_length)
    far_span_length = SIDE_STEPS * FAR_DILATION
    needed = -(-far_span_length // length)
    lower_blocks = collect(pairs[2], needed, 1)
    upper_blocks = collect(pairs[2], needed, -1)
    columns = pairs[2].shape[2]
    lower_flat = jnp.moveaxis(lower_blocks[::-1], 0, 1).reshape(2, needed * length, columns)
    upper_flat = jnp.moveaxis(upper_blocks, 0, 1).reshape(2, needed * length, columns)
    far_full = jnp.concatenate([lower_flat, pairs[2], upper_flat], axis=1)
    extended = (first_ext, middle_ext, far_full)
    outputs = []
    log_sums = []
    for group_idx in range(3):
        group_out, log_sum = banded(
            query_list[group_idx],
            extended[group_idx][0],
            extended[group_idx][1],
            group_dilations[group_idx],
            offset_pos,
            seq_len,
        )
        outputs.append(group_out)
        log_sums.append(log_sum)
    merge_w = jax.nn.softmax(jnp.stack(log_sums, axis=0), axis=0)
    heads = columns // HEAD_DIM
    stacked = jnp.stack(outputs, axis=0).reshape(3, length, heads, HEAD_DIM)
    merged = (
        jnp.sum(merge_w[..., None] * stacked, axis=0).reshape(length, columns).astype(jnp.bfloat16)
    )
    mixed = jnp.dot(
        lax.all_gather(merged, "tp", axis=1, tiled=True),
        out_weight,
        preferred_element_type=jnp.float32,
    )
    return mixed.astype(jnp.bfloat16)


def remote(src, dst, send_sem, recv_sem, axis, target):
    return pltpu.make_async_remote_copy(
        src_ref=src,
        dst_ref=dst,
        send_sem=send_sem,
        recv_sem=recv_sem,
        device_id={axis: target},
        device_id_type=MESH,
    )


def head_mask(columns, head):
    lane = lax.broadcasted_iota(jnp.int32, (1, columns), 1)
    return (lane // HEAD_DIM == head).astype(jnp.float32)


def attend(queries, keys, values, bias):
    rows, columns = queries.shape
    heads = columns // HEAD_DIM
    masks = [head_mask(columns, head) for head in range(heads)]
    stacked = jnp.concatenate([queries * mask.astype(jnp.bfloat16) for mask in masks], axis=0)
    scores = lax.dot_general(
        stacked, keys, (((1,), (1,)), ((), ())), preferred_element_type=jnp.float32
    )
    width = keys.shape[0]
    scores = (scores.reshape(heads, rows, width) + bias[None]).reshape(heads * rows, width)
    row_max = jnp.max(scores, axis=-1, keepdims=True)
    expo = jnp.exp(scores - row_max)
    denom = jnp.sum(expo, axis=-1, keepdims=True)
    summed = jnp.dot(expo.astype(jnp.bfloat16), values, preferred_element_type=jnp.float32)
    summed = summed / denom
    lse = row_max + jnp.log(denom)
    parts = [slice(head * rows, (head + 1) * rows) for head in range(heads)]
    out = sum(summed[part] * mask for part, mask in zip(parts, masks))
    return out, [lse[part] for part in parts]


def packed_lse(lses):
    heads = len(lses)
    lane = lax.broadcasted_iota(jnp.int32, (1, 128), 1)
    spread = sum(lse * (lane % heads == head).astype(jnp.float32) for head, lse in enumerate(lses))
    total = jnp.zeros_like(spread)
    for term in range(3):
        rounded = spread.astype(jnp.bfloat16).astype(jnp.float32)
        total = total + rounded * (lane // heads == term).astype(jnp.float32)
        spread = spread - rounded
    return total.astype(jnp.bfloat16)


def band_bias(rows, width, offset, low, high):
    query = lax.broadcasted_iota(jnp.int32, (rows, width), 0)
    key = lax.broadcasted_iota(jnp.int32, (rows, width), 1)
    step = key + offset - query
    keep = (step >= -SIDE_STEPS) & (step <= SIDE_STEPS) & (key >= low) & (key < high)
    return jnp.where(keep, 0.0, -1e30)


def permutation(length, dilation, inverse):
    row = lax.broadcasted_iota(jnp.int32, (length, length), 1 if inverse else 0)
    column = lax.broadcasted_iota(jnp.int32, (length, length), 0 if inverse else 1)
    steps = length // dilation
    source = (row % steps) * dilation + row // steps
    return (source == column).astype(jnp.float32).astype(jnp.bfloat16)


def fused_kernel(
    n, m, tokens_hbm, query_hbm, key_hbm, value_hbm, out_hbm, table_hbm, base_ref, result_ref,
    tokens, weights, out_weight, table, kv_first, kv_middle, far_send, far_recv,
    back_send, back_recv, merged_all, load_sem, weight_sem, local_sem,
    near_send_sem, near_recv_sem, far_send_sem, far_recv_sem, back_send_sem, back_recv_sem,
    tp_send_sem, tp_recv_sem,
):
    me = lax.axis_index("sp")
    mine = lax.axis_index("tp")
    length, columns = tokens.shape[0], weights.shape[-1]
    half = HEAD_DIM // 2
    classes = FAR_DILATION // n
    halo = SIDE_STEPS

    loads = [
        pltpu.make_async_copy(tokens_hbm, tokens, load_sem.at[0]),
        pltpu.make_async_copy(table_hbm, table, load_sem.at[1]),
        pltpu.make_async_copy(out_hbm, out_weight, load_sem.at[2]),
    ]
    weight_loads = {}
    for group in (2, 1, 0):
        for kind, source in ((1, key_hbm), (2, value_hbm), (0, query_hbm)):
            slot = group * 3 + kind
            weight_loads[group, kind] = pltpu.make_async_copy(
                source.at[group], weights.at[slot], weight_sem.at[slot]
            )
    loads[0].start()
    loads[1].start()
    for kind in (1, 2, 0):
        weight_loads[2, kind].start()
    later_loads = [weight_loads[group, kind] for group in (0, 1) for kind in (1, 2)]
    later_loads += [weight_loads[1, 0], weight_loads[0, 0], loads[2]]

    barrier = pltpu.get_barrier_semaphore()
    for distance in range(1, n):
        pl.semaphore_signal(
            barrier, inc=1, device_id={"sp": lax.rem(me + distance, n)}, device_id_type=MESH
        )
    for distance in range(1, m):
        pl.semaphore_signal(
            barrier, inc=1, device_id={"tp": lax.rem(mine + distance, m)}, device_id_type=MESH
        )

    @pl.when(me == 0)
    def _():
        kv_first[:, :halo] = jnp.zeros((2, halo, columns), jnp.bfloat16)
        kv_middle[:, :, 0] = jnp.zeros_like(kv_middle[:, :, 0])

    @pl.when(me == n - 1)
    def _():
        kv_first[:, halo + length :] = jnp.zeros((2, halo, columns), jnp.bfloat16)
        kv_middle[:, :, 2] = jnp.zeros_like(kv_middle[:, :, 2])

    loads[1].wait()
    base_cos = base_ref[0, pl.ds(me, 1), :]
    base_sin = base_ref[1, pl.ds(me, 1), :]
    cosine = base_cos * table[0] - base_sin * table[1]
    sine = base_sin * table[0] + base_cos * table[1]
    wide = columns // cosine.shape[1]
    lane = lax.broadcasted_iota(jnp.int32, (1, columns), 1)
    first_half = lane % HEAD_DIM < half
    cosine = jnp.concatenate([cosine] * wide, axis=1)
    sine = jnp.concatenate([sine] * wide, axis=1) * jnp.where(first_half, -1.0, 1.0)
    far_order = permutation(length, FAR_DILATION, False)
    middle_order = permutation(length, MIDDLE_DILATION, False)
    loads[0].wait()

    def project(group, kind):
        weight_loads[group, kind].wait()
        product = jnp.dot(
            tokens[...], weights[group * 3 + kind], preferred_element_type=jnp.float32
        )
        if kind < 2:
            later = pltpu.roll(product, columns - half, 1)
            earlier = pltpu.roll(product, half, 1)
            product = product * cosine + jnp.where(first_half, later, earlier) * sine
        if kind == 0:
            product = product * HEAD_DIM ** (-0.5)
        return product.astype(jnp.bfloat16)

    def ordered(order, block):
        return jnp.dot(order, block, preferred_element_type=jnp.float32).astype(jnp.bfloat16)

    far_copies = []
    for kind in (1, 2, 0):
        far_send[kind] = ordered(far_order, project(2, kind)).reshape(far_send.shape[1:])
        for load in later_loads[:3]:
            load.start()
        later_loads = later_loads[3:]
        if kind == 1:
            pl.semaphore_wait(barrier, n - 1 + m - 1)
        for distance in range(1, n):
            target = lax.rem(me + distance, n)
            copy = remote(
                far_send.at[kind, pl.ds(target * classes, classes)],
                far_recv.at[kind, :, me],
                far_send_sem.at[kind, distance],
                far_recv_sem.at[kind, distance],
                "sp",
                target,
            )
            copy.start()
            far_copies.append(copy)
    far_own = pltpu.make_async_copy(
        far_send.at[:, pl.ds(me * classes, classes)], far_recv.at[:, :, me], local_sem.at[0]
    )
    far_own.start()

    middle_up = remote(
        kv_middle.at[:, :, 1], kv_middle.at[:, :, 0],
        near_send_sem.at[0], near_recv_sem.at[0], "sp", lax.rem(me + 1, n),
    )
    middle_down = remote(
        kv_middle.at[:, :, 1], kv_middle.at[:, :, 2],
        near_send_sem.at[1], near_recv_sem.at[1], "sp", lax.rem(me + n - 1, n),
    )
    first_up = remote(
        kv_first.at[:, pl.ds(length, halo)], kv_first.at[:, pl.ds(0, halo)],
        near_send_sem.at[2], near_recv_sem.at[2], "sp", lax.rem(me + 1, n),
    )
    first_down = remote(
        kv_first.at[:, pl.ds(halo, halo)], kv_first.at[:, pl.ds(halo + length, halo)],
        near_send_sem.at[3], near_recv_sem.at[3], "sp", lax.rem(me + n - 1, n),
    )

    for kind in (1, 2):
        kv_first[kind - 1, halo : halo + length] = project(0, kind)

    @pl.when(me < n - 1)
    def _():
        first_up.start()

    @pl.when(me > 0)
    def _():
        first_down.start()

    for kind in (1, 2):
        kv_middle[kind - 1, :, 1] = ordered(middle_order, project(1, kind)).reshape(
            MIDDLE_DILATION, length // MIDDLE_DILATION, columns
        )
    @pl.when(me < n - 1)
    def _():
        middle_up.start()

    @pl.when(me > 0)
    def _():
        middle_down.start()

    middle_queries = ordered(middle_order, project(1, 0))
    first_queries = project(0, 0)

    far_own.wait()
    for copy in far_copies:
        copy.wait()
    class_len = n * (length // FAR_DILATION)
    far_bias = band_bias(class_len, class_len, 0, 0, class_len)
    for index in range(classes):
        queries, keys, values = (
            far_recv[kind, index].reshape(class_len, columns) for kind in range(3)
        )
        out, lses = attend(queries, keys, values, far_bias)
        back_send[index, :, :, :columns] = out.astype(jnp.bfloat16).reshape(n, -1, columns)
        back_send[index, :, :, columns:] = packed_lse(lses).reshape(n, -1, 128)
    back_copies = []
    for distance in range(1, n):
        target = lax.rem(me + distance, n)
        copy = remote(
            back_send.at[:, target],
            back_recv.at[pl.ds(me * classes, classes)],
            back_send_sem.at[distance],
            back_recv_sem.at[distance],
            "sp",
            target,
        )
        copy.start()
        back_copies.append(copy)
    back_own = pltpu.make_async_copy(
        back_send.at[:, me], back_recv.at[pl.ds(me * classes, classes)], local_sem.at[1]
    )
    back_own.start()

    @pl.when(me < n - 1)
    def _():
        first_up.wait_send()
        first_down.wait_recv()

    @pl.when(me > 0)
    def _():
        first_down.wait_send()
        first_up.wait_recv()

    tile = 2 * halo
    first_outs = []
    first_lses = []
    for start in range(0, length, tile):
        width = tile + 2 * halo
        low = halo - start - me * length
        high = halo - start + (n - me) * length
        out, lses = attend(
            first_queries[start : start + tile],
            kv_first[0, start : start + width],
            kv_first[1, start : start + width],
            band_bias(tile, width, -halo, low, high),
        )
        first_outs.append(out)
        first_lses.append(
            sum(lse * head_mask(columns, head) for head, lse in enumerate(lses))
        )
    first_out = jnp.concatenate(first_outs, axis=0)
    first_lse = jnp.concatenate(first_lses, axis=0)

    @pl.when(me < n - 1)
    def _():
        middle_up.wait_send()
        middle_down.wait_recv()

    @pl.when(me > 0)
    def _():
        middle_down.wait_send()
        middle_up.wait_recv()

    steps = length // MIDDLE_DILATION
    low = jnp.where(me == 0, steps, 0)
    high = jnp.where(me == n - 1, 2 * steps, 3 * steps)
    middle_bias = band_bias(steps, 3 * steps, -steps, low, high)
    middle_parts = []
    for index in range(MIDDLE_DILATION):
        out, lses = attend(
            middle_queries[index * steps : (index + 1) * steps],
            kv_middle[0, index].reshape(3 * steps, columns),
            kv_middle[1, index].reshape(3 * steps, columns),
            middle_bias,
        )
        middle_parts.append(
            jnp.concatenate([out.astype(jnp.bfloat16), packed_lse(lses)], axis=1)
        )

    heads = columns // HEAD_DIM
    term = lax.broadcasted_iota(jnp.int32, (128, columns), 0)
    column = lax.broadcasted_iota(jnp.int32, (128, columns), 1)
    spread = (term % heads == column // HEAD_DIM) & (term < 3 * heads)
    spread = spread.astype(jnp.float32).astype(jnp.bfloat16)

    def natural(dilation, block):
        block = jnp.dot(
            permutation(length, dilation, True), block, preferred_element_type=jnp.float32
        )
        lse = jnp.dot(
            block[:, columns:].astype(jnp.bfloat16), spread, preferred_element_type=jnp.float32
        )
        return block[:, :columns], lse

    middle_out, middle_lse = natural(MIDDLE_DILATION, jnp.concatenate(middle_parts, axis=0))

    back_own.wait()
    for copy in back_copies:
        copy.wait()
    far_out, far_lse = natural(
        FAR_DILATION, back_recv[...].reshape(length, back_recv.shape[2])
    )

    top = jnp.maximum(jnp.maximum(first_lse, middle_lse), far_lse)
    first_w = jnp.exp(first_lse - top)
    middle_w = jnp.exp(middle_lse - top)
    far_w = jnp.exp(far_lse - top)
    merged = (first_w * first_out + middle_w * middle_out + far_w * far_out) / (
        first_w + middle_w + far_w
    )
    merged_all[0] = merged.astype(jnp.bfloat16)

    chips = m // 2
    sibling = mine + 1 - 2 * lax.rem(mine, 2)
    piece = length // 2

    def hand(part, source, slot, target):
        rows = pl.ds(part * piece, piece)
        copy = remote(
            merged_all.at[source, rows],
            merged_all.at[slot, rows],
            tp_send_sem.at[part, slot],
            tp_recv_sem.at[part, slot],
            "tp",
            target,
        )
        copy.start()
        return copy

    copies = {}
    for part in range(2):
        for chip in range(1, chips):
            copies[part, chip] = hand(part, 0, chip, lax.rem(mine + 2 * chip, m))
    for part in range(2):
        copies[part, chips] = hand(part, 0, chips, sibling)
    loads[2].wait()

    def term(part, slot):
        chip = slot % chips
        owner = lax.rem((mine if slot < chips else sibling) - 2 * chip + m, m)
        rows = pl.ds(pl.multiple_of(owner * columns, columns), columns)
        return jnp.dot(
            merged_all[slot, part * piece : (part + 1) * piece],
            out_weight[rows, :],
            preferred_element_type=jnp.float32,
        )

    totals = [term(part, 0) for part in range(2)]
    for part in range(2):
        for chip in range(1, chips):
            copies[part, chip].wait()
            copies[part, chips + chip] = hand(part, chip, chips + chip, sibling)
        copies[part, chips].wait()
        totals[part] = totals[part] + term(part, chips)
        for chip in range(1, chips):
            totals[part] = totals[part] + term(part, chip)
    for part in range(2):
        for chip in range(1, chips):
            copies[part, chips + chip].wait()
            totals[part] = totals[part] + term(part, chips + chip)
        result_ref[part * piece : (part + 1) * piece] = totals[part].astype(result_ref.dtype)


def turn_tables(n, length):
    half = HEAD_DIM // 2
    inverse = 1.0 / 10000.0 ** (np.arange(half, dtype=np.float32) * np.float32(2.0) / HEAD_DIM)
    inverse = np.tile(inverse.astype(np.float64), 128 // half)[None]
    inner = np.arange(length)[:, None] * inverse
    outer = (np.arange(n) * length)[:, None] * inverse
    table = np.stack([np.cos(inner), np.sin(inner)]).astype(np.float32)
    base = np.stack([np.cos(outer), np.sin(outer)]).astype(np.float32)
    return table, base


def fused(n, m, tokens, query_weight, key_weight, value_weight, out_weight):
    length, width = tokens.shape
    columns = query_weight.shape[2]
    table, base = turn_tables(n, length)
    steps = length // FAR_DILATION
    classes = FAR_DILATION // n
    kept = columns + 128
    bf16 = jnp.bfloat16
    hbm = pl.BlockSpec(memory_space=pl.ANY)
    vmem = pl.BlockSpec(memory_space=pltpu.VMEM)
    dma = pltpu.SemaphoreType.DMA
    return pl.pallas_call(
        functools.partial(fused_kernel, n, m),
        out_shape=pltpu.VMEM((length, out_weight.shape[1]), bf16),
        in_specs=[hbm] * 6 + [vmem],
        out_specs=vmem,
        scratch_shapes=[
            pltpu.VMEM((length, width), bf16),
            pltpu.VMEM((9, width, columns), bf16),
            pltpu.VMEM(out_weight.shape, bf16),
            pltpu.VMEM(table.shape, jnp.float32),
            pltpu.VMEM((2, length + 2 * SIDE_STEPS, columns), bf16),
            pltpu.VMEM((2, MIDDLE_DILATION, 3, length // MIDDLE_DILATION, columns), bf16),
            pltpu.VMEM((3, FAR_DILATION, steps, columns), bf16),
            pltpu.VMEM((3, classes, n, steps, columns), bf16),
            pltpu.VMEM((classes, n, steps, kept), bf16),
            pltpu.VMEM((FAR_DILATION, steps, kept), bf16),
            pltpu.VMEM((m, length, columns), bf16),
            dma((3,)),
            dma((9,)),
            dma((2,)),
            dma((4,)),
            dma((4,)),
            dma((3, n)),
            dma((3, n)),
            dma((n,)),
            dma((n,)),
            dma((2, m)),
            dma((2, m)),
        ],
        compiler_params=pltpu.CompilerParams(
            collective_id=0, has_side_effects=True, vmem_limit_bytes=60 * 1024 * 1024
        ),
    )(tokens, query_weight, key_weight, value_weight, out_weight, jnp.asarray(table), jnp.asarray(base))


def planned(n, m, *arrays):
    length, columns = arrays[0].shape[0], arrays[1].shape[2]
    fits = (
        n > 1
        and m % 2 == 0
        and FAR_DILATION % n == 0
        and length == SIDE_STEPS * MIDDLE_DILATION
        and length % (FAR_DILATION * 16) == 0
        and columns % 128 == 0
        and 3 * (columns // HEAD_DIM) <= 128
    )
    if fits:
        return fused(n, m, *arrays)
    return per_device(*arrays)


def solution(mesh):
    placed = (
        P("sp", None),
        P(None, None, "tp"),
        P(None, None, "tp"),
        P(None, None, "tp"),
        P(None, "tp"),
    )
    return jax.shard_map(
        functools.partial(planned, mesh.shape["sp"], mesh.shape["tp"]),
        mesh=mesh,
        in_specs=placed,
        out_specs=P("sp", "tp"),
        check_vma=False,
    )
```

```python
import functools
import math

import jax
import numpy as np
import jax.numpy as jnp
from jax import lax
from jax.experimental import pallas as pl
from jax.experimental.pallas import tpu as pltpu
from jax.sharding import PartitionSpec as P

HEAD_DIM = 64
SIDE_STEPS = 64
MIDDLE_DILATION = 4
FAR_DILATION = 16
MESH = pl.DeviceIdType.MESH


def shifted(block, axis, distance):
    devices = range(lax.axis_size(axis))
    route = [(i - distance, i) for i in devices if i - distance in devices]
    return lax.ppermute(block, axis, route)


def with_halo(block, sides, width):
    for axis, dim in sides:
        count = lax.axis_size(axis)
        forward = [(i, i + 1) for i in range(count - 1)]
        backward = [(target, source) for source, target in forward]
        low = lax.ppermute(
            lax.slice_in_dim(block, block.shape[dim] - width, None, axis=dim), axis, forward
        )
        high = lax.ppermute(lax.slice_in_dim(block, 0, width, axis=dim), axis, backward)
        block = jnp.concatenate([low, block, high], axis=dim)
    return block


def rotate(projected, offset_pos):
    length, columns = projected.shape
    heads = columns // HEAD_DIM
    half = HEAD_DIM // 2
    positions = (offset_pos + jnp.arange(length)).astype(jnp.float32)
    inverse = 1.0 / 10000.0 ** (jnp.arange(half, dtype=jnp.float32) * 2.0 / HEAD_DIM)
    angles = positions[:, None] * inverse[None, :]
    angles = jnp.concatenate([angles, angles], axis=-1)
    cosine_table = jnp.cos(angles)[:, None, :]
    sine = jnp.sin(angles)[:, None, :]
    shaped = projected.reshape(length, heads, HEAD_DIM)
    turned = jnp.concatenate([-shaped[..., half:], shaped[..., :half]], axis=-1)
    return (shaped * cosine_table + turned * sine).reshape(length, columns)


def banded(queries, key_ext, value_ext, dilation, offset_pos, seq_len):
    length, columns = queries.shape
    heads = columns // HEAD_DIM
    class_len = length // dilation
    block_len = math.gcd(SIDE_STEPS, class_len)
    blocks = class_len // block_len
    extra = 2 * SIDE_STEPS // block_len
    query_blocks = queries.reshape(blocks, block_len, dilation, heads, HEAD_DIM)
    key_blocks = key_ext.reshape(blocks + extra, block_len, dilation, heads, HEAD_DIM)
    value_blocks = value_ext.reshape(blocks + extra, block_len, dilation, heads, HEAD_DIM)
    key_win = jnp.concatenate(
        [key_blocks[shift_idx : shift_idx + blocks] for shift_idx in range(extra + 1)], axis=1
    )
    value_win = jnp.concatenate(
        [value_blocks[shift_idx : shift_idx + blocks] for shift_idx in range(extra + 1)], axis=1
    )
    scores = jnp.einsum(
        "bqrhe,bkrhe->brhqk", query_blocks, key_win, preferred_element_type=jnp.float32
    )
    scores = scores * HEAD_DIM ** (-0.5)
    width_keys = key_win.shape[1]
    relative = jnp.arange(width_keys)[None, :] - jnp.arange(block_len)[:, None]
    within = (relative >= 0) & (relative <= 2 * SIDE_STEPS)
    key_rows = jnp.arange(blocks)[:, None] * block_len + jnp.arange(width_keys)[None, :]
    spots = (
        offset_pos
        - SIDE_STEPS * dilation
        + dilation * key_rows[:, :, None]
        + jnp.arange(dilation)[None, None, :]
    )
    inside = (spots >= 0) & (spots < seq_len)
    allowed = within[None, None, None] & jnp.transpose(inside, (0, 2, 1))[:, :, None, None, :]
    scores = jnp.where(allowed, scores, -1e30)
    row_max = jnp.max(scores, axis=-1, keepdims=True)
    expo = jnp.exp(scores - row_max)
    denom = jnp.sum(expo, axis=-1)
    probs = expo.astype(jnp.bfloat16)
    summed = jnp.einsum("brhqk,bkrhe->bqrhe", probs, value_win, preferred_element_type=jnp.float32)
    group_out = summed / jnp.transpose(denom, (0, 3, 1, 2))[..., None]
    log_sum = row_max[..., 0] + jnp.log(denom)
    log_sum = jnp.transpose(log_sum, (0, 3, 1, 2)).reshape(length, heads)
    return (group_out.reshape(length, columns), log_sum)


def collect(own_block, needed, direction):
    collected = own_block[None]
    while collected.shape[0] < needed + 1:
        stride = collected.shape[0]
        to_send = min(stride, needed + 1 - stride)
        arrived = shifted(collected[:to_send], "sp", direction * stride)
        collected = jnp.concatenate([collected, arrived], axis=0)
    return collected[1:]


def per_device(tokens, query_weight, key_weight, value_weight, out_weight):
    length = tokens.shape[0]
    offset_pos = lax.axis_index("sp") * length
    seq_len = lax.axis_size("sp") * length
    group_dilations = (1, MIDDLE_DILATION, FAR_DILATION)
    query_list = []
    pairs = []
    for group_idx in range(3):
        queries = rotate(
            jnp.dot(tokens, query_weight[group_idx], preferred_element_type=jnp.float32), offset_pos
        )
        keys_here = rotate(
            jnp.dot(tokens, key_weight[group_idx], preferred_element_type=jnp.float32), offset_pos
        )
        values_here = jnp.dot(tokens, value_weight[group_idx], preferred_element_type=jnp.float32)
        query_list.append(queries.astype(jnp.bfloat16))
        pairs.append(
            jnp.stack([keys_here.astype(jnp.bfloat16), values_here.astype(jnp.bfloat16)], axis=0)
        )
    middle_span_length = SIDE_STEPS * MIDDLE_DILATION
    first_ext = with_halo(pairs[0], (("sp", 1),), SIDE_STEPS)
    middle_ext = with_halo(pairs[1], (("sp", 1),), middle_span_length)
    far_span_length = SIDE_STEPS * FAR_DILATION
    needed = -(-far_span_length // length)
    lower_blocks = collect(pairs[2], needed, 1)
    upper_blocks = collect(pairs[2], needed, -1)
    columns = pairs[2].shape[2]
    lower_flat = jnp.moveaxis(lower_blocks[::-1], 0, 1).reshape(2, needed * length, columns)
    upper_flat = jnp.moveaxis(upper_blocks, 0, 1).reshape(2, needed * length, columns)
    far_full = jnp.concatenate([lower_flat, pairs[2], upper_flat], axis=1)
    extended = (first_ext, middle_ext, far_full)
    outputs = []
    log_sums = []
    for group_idx in range(3):
        group_out, log_sum = banded(
            query_list[group_idx],
            extended[group_idx][0],
            extended[group_idx][1],
            group_dilations[group_idx],
            offset_pos,
            seq_len,
        )
        outputs.append(group_out)
        log_sums.append(log_sum)
    merge_w = jax.nn.softmax(jnp.stack(log_sums, axis=0), axis=0)
    heads = columns // HEAD_DIM
    stacked = jnp.stack(outputs, axis=0).reshape(3, length, heads, HEAD_DIM)
    merged = (
        jnp.sum(merge_w[..., None] * stacked, axis=0).reshape(length, columns).astype(jnp.bfloat16)
    )
    mixed = jnp.dot(
        lax.all_gather(merged, "tp", axis=1, tiled=True),
        out_weight,
        preferred_element_type=jnp.float32,
    )
    return mixed.astype(jnp.bfloat16)


def remote(src, dst, send_sem, recv_sem, axis, target):
    return pltpu.make_async_remote_copy(
        src_ref=src,
        dst_ref=dst,
        send_sem=send_sem,
        recv_sem=recv_sem,
        device_id={axis: target},
        device_id_type=MESH,
    )


def head_mask(columns, head):
    lane = lax.broadcasted_iota(jnp.int32, (1, columns), 1)
    return (lane // HEAD_DIM == head).astype(jnp.float32)


def attend(queries, keys, values, bias):
    rows, columns = queries.shape
    heads = columns // HEAD_DIM
    masks = [head_mask(columns, head) for head in range(heads)]
    stacked = jnp.concatenate([queries * mask.astype(jnp.bfloat16) for mask in masks], axis=0)
    scores = lax.dot_general(
        stacked, keys, (((1,), (1,)), ((), ())), preferred_element_type=jnp.float32
    )
    width = keys.shape[0]
    scores = (scores.reshape(heads, rows, width) + bias[None]).reshape(heads * rows, width)
    row_max = jnp.max(scores, axis=-1, keepdims=True)
    expo = jnp.exp(scores - row_max)
    denom = jnp.sum(expo, axis=-1, keepdims=True)
    summed = jnp.dot(expo.astype(jnp.bfloat16), values, preferred_element_type=jnp.float32)
    summed = summed / denom
    lse = row_max + jnp.log(denom)
    parts = [slice(head * rows, (head + 1) * rows) for head in range(heads)]
    out = sum(summed[part] * mask for part, mask in zip(parts, masks))
    return out, [lse[part] for part in parts]


def packed_lse(lses):
    heads = len(lses)
    lane = lax.broadcasted_iota(jnp.int32, (1, 128), 1)
    spread = sum(lse * (lane % heads == head).astype(jnp.float32) for head, lse in enumerate(lses))
    total = jnp.zeros_like(spread)
    for term in range(3):
        rounded = spread.astype(jnp.bfloat16).astype(jnp.float32)
        total = total + rounded * (lane // heads == term).astype(jnp.float32)
        spread = spread - rounded
    return total.astype(jnp.bfloat16)


def in_terms(block):
    terms = []
    for _ in range(3):
        rounded = block.astype(jnp.bfloat16)
        terms.append(rounded)
        block = block - rounded.astype(jnp.float32)
    return jnp.concatenate(terms, axis=1)


def band_bias(rows, width, offset, low, high, stride=1):
    query = lax.broadcasted_iota(jnp.int32, (rows, width), 0)
    key = lax.broadcasted_iota(jnp.int32, (rows, width), 1)
    query = (query % (rows // stride)) * stride + query // (rows // stride)
    step = key + offset - query
    keep = (step >= -SIDE_STEPS) & (step <= SIDE_STEPS) & (key >= low) & (key < high)
    return jnp.where(keep, 0.0, -1e30)


def one_hot(size, source_of_row):
    row = lax.broadcasted_iota(jnp.int32, (size, size), 0)
    column = lax.broadcasted_iota(jnp.int32, (size, size), 1)
    return (source_of_row(row) == column).astype(jnp.float32).astype(jnp.bfloat16)


def scope(name):
    return jax.named_scope(name)


def fused_kernel(
    n, m, tokens_hbm, query_hbm, key_hbm, value_hbm, out_hbm, table_hbm, base_hbm, result_ref,
    tokens, weights, out_weight, table, base, kv_first, mid_kv, mid_q, mid_send, mid_ret,
    mid_back, far_send, far_recv, back_send, back_recv, lse_send, lse_recv, merged_all,
    result_wide, load_sem, weight_sem, local_sem, first_send_sem, first_recv_sem,
    pair_send_sem, pair_recv_sem, hop_send_sem, hop_recv_sem, ret_send_sem, ret_recv_sem,
    far_send_sem, far_recv_sem, back_send_sem, back_recv_sem, lse_send_sem, lse_recv_sem,
    tp_send_sem, tp_recv_sem,
):
    me = lax.axis_index("sp")
    mine = lax.axis_index("tp")
    side = lax.rem(me, 2)
    partner = me + 1 - 2 * side
    length, columns = tokens.shape[0], weights.shape[-1]
    depth = tokens.shape[1]
    heads = columns // HEAD_DIM
    half = HEAD_DIM // 2
    classes = FAR_DILATION // n
    far_steps = length // FAR_DILATION
    halo = SIDE_STEPS
    steps = length // MIDDLE_DILATION
    piece = length // 2

    chunk = depth // 2
    token_loads = []
    first_loads = []
    for index in range(2):
        part = pl.ds(index * chunk, chunk)
        token_loads.append(
            pltpu.make_async_copy(tokens_hbm.at[:, part], tokens.at[:, part], load_sem.at[index])
        )
        first_loads.append(
            pltpu.make_async_copy(
                key_hbm.at[2, part], weights.at[2 * 3 + 1, part], load_sem.at[2 + index]
            )
        )
    table_load = pltpu.make_async_copy(table_hbm, table, load_sem.at[4])
    base_load = pltpu.make_async_copy(base_hbm, base, load_sem.at[5])
    out_load = pltpu.make_async_copy(out_hbm, out_weight, load_sem.at[6])
    weight_loads = {}
    for group in (2, 1, 0):
        for kind, source in ((1, key_hbm), (2, value_hbm), (0, query_hbm)):
            slot = group * 3 + kind
            if (group, kind) == (2, 1):
                continue
            weight_loads[group, kind] = pltpu.make_async_copy(
                source.at[group], weights.at[slot], weight_sem.at[slot]
            )
    token_loads[0].start()
    first_loads[0].start()
    base_load.start()
    table_load.start()
    token_loads[1].start()
    first_loads[1].start()
    weight_loads[2, 2].start()
    weight_loads[2, 0].start()
    later_loads = [weight_loads[group, kind] for group in (1, 0) for kind in (1, 2, 0)]
    later_loads.append(out_load)

    barrier = pltpu.get_barrier_semaphore()
    for distance in range(1, n):
        pl.semaphore_signal(
            barrier, inc=1, device_id={"sp": lax.rem(me + distance, n)}, device_id_type=MESH
        )
    for distance in range(1, m):
        pl.semaphore_signal(
            barrier, inc=1, device_id={"tp": lax.rem(mine + distance, m)}, device_id_type=MESH
        )

    far_order = one_hot(
        length, lambda row: (row % far_steps) * FAR_DILATION + row // far_steps
    )
    middle_order = one_hot(
        length,
        lambda row: (row % steps) * MIDDLE_DILATION + (row // steps + 2 * side) % MIDDLE_DILATION,
    )
    tile = 2 * halo
    first_order = one_hot(
        length, lambda row: row // tile * tile + (row % halo) * 2 + row % tile // halo
    )
    lane = lax.broadcasted_iota(jnp.int32, (1, columns), 1)
    first_half = lane % HEAD_DIM < half

    def product_of(slot, low, size):
        return jnp.dot(
            tokens[:, low : low + size],
            weights[slot, low : low + size],
            preferred_element_type=jnp.float32,
        )

    def rolled(block, shift):
        return jnp.concatenate(
            [pltpu.roll(block[:, at : at + 128], shift, 1) for at in range(0, columns, 128)], axis=1
        )

    def turned(product, kind):
        if kind < 2:
            later = rolled(product, 128 - half)
            earlier = rolled(product, half)
            product = product * cosine + jnp.where(first_half, later, earlier) * sine
        if kind == 0:
            product = product * HEAD_DIM ** (-0.5)
        return product.astype(jnp.bfloat16)

    def project(group, kind):
        slot = group * 3 + kind
        weight_loads[group, kind].wait()
        return turned(product_of(slot, 0, depth), kind)

    def ordered(order, block):
        return jnp.dot(order, block, preferred_element_type=jnp.float32).astype(jnp.bfloat16)

    with scope("w_load0"):
        token_loads[0].wait()
        first_loads[0].wait()
    first_product = product_of(7, 0, chunk)
    with scope("w_load1"):
        base_load.wait()
        table_load.wait()
        token_loads[1].wait()
        first_loads[1].wait()
    first_product = first_product + product_of(7, chunk, chunk)
    base_cos = base[0, pl.ds(me, 1), :]
    base_sin = base[1, pl.ds(me, 1), :]
    cosine = base_cos * table[0] - base_sin * table[1]
    sine = base_sin * table[0] + base_cos * table[1]
    wide = columns // cosine.shape[1]
    cosine = jnp.concatenate([cosine] * wide, axis=1)
    sine = jnp.concatenate([sine] * wide, axis=1) * jnp.where(first_half, -1.0, 1.0)

    far_copies = []
    for kind in (1, 2, 0):
        with scope(f"p_far{kind}"):
            block = turned(first_product, 1) if kind == 1 else project(2, kind)
            far_send[kind] = ordered(far_order, block).reshape(far_send.shape[1:])
        for load in later_loads[:3]:
            load.start()
        later_loads = later_loads[3:]
        if kind == 1:
            with scope("w_barrier"):
                pl.semaphore_wait(barrier, n - 1 + m - 1)
        for distance in range(1, n):
            target = lax.rem(me + distance, n)
            copy = remote(
                far_send.at[kind, pl.ds(target * classes, classes)],
                far_recv.at[kind, :, me],
                far_send_sem.at[kind, distance],
                far_recv_sem.at[kind, distance],
                "sp",
                target,
            )
            copy.start()
            far_copies.append(copy)
    far_own = pltpu.make_async_copy(
        far_send.at[:, pl.ds(me * classes, classes)], far_recv.at[:, :, me], local_sem.at[0]
    )
    far_own.start()

    pair_copies = []
    for kind in (1, 2, 0):
        with scope(f"p_mid{kind}"):
            block = ordered(middle_order, project(1, kind)).reshape(2, 2, steps, columns)
            if kind == 0:
                mid_q[:, pl.ds(side, 1)] = block[0][:, None]
                landing = mid_q.at[:, side]
            else:
                mid_kv[kind - 1, :, pl.ds(1 + side, 1)] = block[0][:, None]
                landing = mid_kv.at[kind - 1, :, 1 + side]
            mid_send[kind] = block[1]
        copy = remote(
            mid_send.at[kind], landing, pair_send_sem.at[kind], pair_recv_sem.at[kind],
            "sp", partner,
        )
        copy.start()
        pair_copies.append(copy)

    for kind in (1, 2):
        with scope(f"p_first{kind}"):
            kv_first[kind - 1, halo : halo + length] = project(0, kind)

    @pl.when(me == 0)
    def _():
        kv_first[:, :halo] = jnp.zeros((2, halo, columns), jnp.bfloat16)

    @pl.when(me == n - 1)
    def _():
        kv_first[:, halo + length :] = jnp.zeros((2, halo, columns), jnp.bfloat16)

    @pl.when(me < 2)
    def _():
        mid_kv[:, :, 0] = jnp.zeros_like(mid_kv[:, :, 0])

    @pl.when(me >= n - 2)
    def _():
        mid_kv[:, :, 3] = jnp.zeros_like(mid_kv[:, :, 3])

    first_up = remote(
        kv_first.at[:, pl.ds(length, halo)], kv_first.at[:, pl.ds(0, halo)],
        first_send_sem.at[0], first_recv_sem.at[0], "sp", lax.rem(me + 1, n),
    )
    first_down = remote(
        kv_first.at[:, pl.ds(halo, halo)], kv_first.at[:, pl.ds(halo + length, halo)],
        first_send_sem.at[1], first_recv_sem.at[1], "sp", lax.rem(me + n - 1, n),
    )

    @pl.when(me < n - 1)
    def _():
        first_up.start()

    @pl.when(me > 0)
    def _():
        first_down.start()

    with scope("p_first0"):
        first_queries = ordered(first_order, project(0, 0))

    hop_up = remote(
        mid_kv.at[:, :, 2], mid_kv.at[:, :, 0],
        hop_send_sem.at[0], hop_recv_sem.at[0], "sp", lax.rem(me + 2, n),
    )
    hop_down = remote(
        mid_kv.at[:, :, 1], mid_kv.at[:, :, 3],
        hop_send_sem.at[1], hop_recv_sem.at[1], "sp", lax.rem(me + n - 2, n),
    )
    with scope("w_pair"):
        pair_copies[0].wait_recv()
        pair_copies[1].wait_recv()

    @pl.when(me < n - 2)
    def _():
        hop_up.start()

    @pl.when(me >= 2)
    def _():
        hop_down.start()

    with scope("w_far"):
        far_own.wait()
        for copy in far_copies:
            copy.wait()
    class_len = n * far_steps
    far_bias = band_bias(class_len, class_len, 0, 0, class_len)
    row16 = lax.broadcasted_iota(jnp.int32, (class_len, 128), 0) % far_steps
    lane16 = lax.broadcasted_iota(jnp.int32, (class_len, 128), 1)
    diagonal = lane16 % far_steps == row16
    back_copies = []
    for index in range(classes):
        with scope(f"c_far{index}"):
            queries, keys, values = (
                far_recv[kind, index].reshape(class_len, columns) for kind in range(3)
            )
            out, lses = attend(queries, keys, values, far_bias)
            back_send[index] = out.astype(jnp.bfloat16).reshape(n, far_steps, columns)
            spread = sum(
                jnp.where(diagonal & (lane16 // far_steps == head), lse, 0.0)
                for head, lse in enumerate(lses)
            )
            lse_send[index] = jnp.sum(spread.reshape(n, far_steps, 128), axis=1, keepdims=True)
        sent = []
        for distance in range(1, n):
            target = lax.rem(me + distance, n)
            for source, landing, send_sem, recv_sem in (
                (back_send, back_recv, back_send_sem, back_recv_sem),
                (lse_send, lse_recv, lse_send_sem, lse_recv_sem),
            ):
                copy = remote(
                    source.at[index, target], landing.at[index, me],
                    send_sem.at[index, distance], recv_sem.at[index, distance], "sp", target,
                )
                copy.start()
                sent.append(copy)
        for which, (source, landing) in enumerate(((back_send, back_recv), (lse_send, lse_recv))):
            copy = pltpu.make_async_copy(
                source.at[index, me], landing.at[index, me], local_sem.at[1 + 2 * index + which]
            )
            copy.start()
            sent.append(copy)
        back_copies.append(sent)

    with scope("w_first"):
        @pl.when(me < n - 1)
        def _():
            first_up.wait_send()
            first_down.wait_recv()

        @pl.when(me > 0)
        def _():
            first_down.wait_send()
            first_up.wait_recv()

    first_outs = []
    first_lses = []
    with scope("c_first"):
        for start in range(0, length, tile):
            width = tile + 2 * halo
            low = halo - start - me * length
            high = halo - start + (n - me) * length
            out, lses = attend(
                first_queries[start : start + tile],
                kv_first[0, start : start + width],
                kv_first[1, start : start + width],
                band_bias(tile, width, -halo, low, high, 2),
            )
            first_outs.append(out)
            first_lses.append(
                sum(lse * head_mask(columns, head) for head, lse in enumerate(lses))
            )

    with scope("w_hop"):
        pair_copies[2].wait_recv()
        for copy in pair_copies:
            copy.wait_send()

        @pl.when(me < n - 2)
        def _():
            hop_up.wait_send()
            hop_down.wait_recv()

        @pl.when(me >= 2)
        def _():
            hop_down.wait_send()
            hop_up.wait_recv()

    low = jnp.where(me < 2, steps, 0)
    high = jnp.where(me >= n - 2, 3 * steps, 4 * steps)
    middle_bias = band_bias(2 * steps, 4 * steps, -steps, low, high)
    ret_copies = []
    for index in range(2):
        with scope(f"c_mid{index}"):
            out, lses = attend(
                mid_q[index].reshape(2 * steps, columns),
                mid_kv[0, index].reshape(4 * steps, columns),
                mid_kv[1, index].reshape(4 * steps, columns),
                middle_bias,
            )
            mid_ret[index] = jnp.concatenate(
                [out.astype(jnp.bfloat16), packed_lse(lses)], axis=1
            ).reshape(2, steps, columns + 128)
        copy = remote(
            mid_ret.at[index, 1 - side], mid_back.at[index],
            ret_send_sem.at[index], ret_recv_sem.at[index], "sp", partner,
        )
        copy.start()
        ret_copies.append(copy)

    term_row = lax.broadcasted_iota(jnp.int32, (128, columns), 0)
    column = lax.broadcasted_iota(jnp.int32, (128, columns), 1)
    middle_spread = (term_row % heads == column // HEAD_DIM) & (term_row < 3 * heads)
    middle_spread = middle_spread.astype(jnp.float32).astype(jnp.bfloat16)
    far_spread = term_row // far_steps == column // HEAD_DIM
    far_spread = far_spread.astype(jnp.float32).astype(jnp.bfloat16)
    far_spread = jnp.concatenate([far_spread] * 3, axis=0)
    middle_natural = one_hot(
        piece, lambda row: row // 2 + steps * ((row % 2 + side) % 2)
    )
    far_natural = one_hot(piece, lambda row: (row % n) * far_steps + row // n)
    position = lax.broadcasted_iota(jnp.int32, (piece, 128), 0) // n
    lane_part = lax.broadcasted_iota(jnp.int32, (piece, 128), 1)
    far_keep = (lane_part % far_steps == position) & (lane_part < heads * far_steps)

    near = []
    for part in range(2):
        with scope(f"w_ret{part}"):
            ret_copies[part].wait()
        with scope(f"c_near{part}"):
            block = jnp.concatenate([mid_ret[part, side], mid_back[part]], axis=0)
            block = jnp.dot(middle_natural, block, preferred_element_type=jnp.float32)
            middle_lse = jnp.dot(
                block[:, columns:].astype(jnp.bfloat16),
                middle_spread,
                preferred_element_type=jnp.float32,
            )
            rows = slice(part * halo, (part + 1) * halo)
            first_out = jnp.concatenate([out[rows] for out in first_outs], axis=0)
            first_lse = jnp.concatenate([lse[rows] for lse in first_lses], axis=0)
            top = jnp.maximum(first_lse, middle_lse)
            first_w = jnp.exp(first_lse - top)
            middle_w = jnp.exp(middle_lse - top)
            near.append(
                (first_w * first_out + middle_w * block[:, :columns], first_w + middle_w, top)
            )

    chips = m // 2
    sibling = mine + 1 - 2 * lax.rem(mine, 2)

    def hand(part, source, slot, target):
        rows = pl.ds(part * piece, piece)
        copy = remote(
            merged_all.at[source, rows],
            merged_all.at[slot, rows],
            tp_send_sem.at[part, slot],
            tp_recv_sem.at[part, slot],
            "tp",
            target,
        )
        copy.start()
        return copy

    def term(part, slot):
        chip = slot % chips
        owner = lax.rem((mine if slot < chips else sibling) - 2 * chip + m, m)
        rows = pl.ds(pl.multiple_of(owner * columns, columns), columns)
        return jnp.dot(
            merged_all[slot, part * piece : (part + 1) * piece],
            out_weight[rows, :],
            preferred_element_type=jnp.float32,
        )

    copies = {}
    totals = []
    with scope("w_outw"):
        out_load.wait()
    for part in range(2):
        with scope(f"w_back{part}"):
            for copy in back_copies[part]:
                copy.wait()
        with scope(f"c_merge{part}"):
            far_out = jnp.dot(
                far_natural,
                back_recv[part].reshape(piece, columns),
                preferred_element_type=jnp.float32,
            )
            lse = jnp.concatenate([lse_recv[part].reshape(n, 128)] * (piece // n), axis=0)
            lse = jnp.where(far_keep, lse, 0.0)
            far_lse = jnp.dot(in_terms(lse), far_spread, preferred_element_type=jnp.float32)
            total, weight, near_top = near[part]
            top = jnp.maximum(near_top, far_lse)
            near_w = jnp.exp(near_top - top)
            far_w = jnp.exp(far_lse - top)
            merged = (near_w * total + far_w * far_out) / (near_w * weight + far_w)
            merged_all[0, part * piece : (part + 1) * piece] = merged.astype(jnp.bfloat16)
        for chip in range(1, chips):
            copies[part, chip] = hand(part, 0, chip, lax.rem(mine + 2 * chip, m))
        copies[part, chips] = hand(part, 0, chips, sibling)
        totals.append(term(part, 0))

    for part in range(2):
        for chip in range(1, chips):
            with scope(f"w_chip{part}"):
                copies[part, chip].wait()
            copies[part, chips + chip] = hand(part, chip, chips + chip, sibling)
        with scope(f"w_sib{part}"):
            copies[part, chips].wait()
        totals[part] = totals[part] + term(part, chips)
        for chip in range(1, chips):
            totals[part] = totals[part] + term(part, chip)
    for part in range(2):
        for chip in range(1, chips):
            with scope(f"w_fwd{part}"):
                copies[part, chips + chip].wait()
            totals[part] = totals[part] + term(part, chips + chip)
        for index in range(result_wide.shape[0]):
            result_wide[index, pl.ds(part, piece, stride=2), :] = totals[part][
                :, index * 128 : (index + 1) * 128
            ]
    for index in range(result_wide.shape[0]):
        result_ref[:, index * 128 : (index + 1) * 128] = result_wide[index].astype(
            result_ref.dtype
        )


def turn_tables(n, length):
    half = HEAD_DIM // 2
    inverse = 1.0 / 10000.0 ** (np.arange(half, dtype=np.float32) * np.float32(2.0) / HEAD_DIM)
    inverse = np.tile(inverse.astype(np.float64), 128 // half)[None]
    inner = np.arange(length)[:, None] * inverse
    outer = (np.arange(n) * length)[:, None] * inverse
    table = np.stack([np.cos(inner), np.sin(inner)]).astype(np.float32)
    base = np.stack([np.cos(outer), np.sin(outer)]).astype(np.float32)
    return table, base


def fused(n, m, tokens, query_weight, key_weight, value_weight, out_weight):
    length, width = tokens.shape
    columns = query_weight.shape[2]
    table, base = turn_tables(n, length)
    steps = length // FAR_DILATION
    span = length // MIDDLE_DILATION
    classes = FAR_DILATION // n
    kept = columns + 128
    bf16 = jnp.bfloat16
    hbm = pl.BlockSpec(memory_space=pl.ANY)
    vmem = pl.BlockSpec(memory_space=pltpu.VMEM)
    dma = pltpu.SemaphoreType.DMA
    return pl.pallas_call(
        functools.partial(fused_kernel, n, m),
        out_shape=pltpu.VMEM((length, out_weight.shape[1]), bf16),
        in_specs=[hbm] * 7,
        out_specs=vmem,
        scratch_shapes=[
            pltpu.VMEM((length, width), bf16),
            pltpu.VMEM((9, width, columns), bf16),
            pltpu.VMEM(out_weight.shape, bf16),
            pltpu.VMEM(table.shape, jnp.float32),
            pltpu.VMEM(base.shape, jnp.float32),
            pltpu.VMEM((2, length + 2 * SIDE_STEPS, columns), bf16),
            pltpu.VMEM((2, 2, 4, span, columns), bf16),
            pltpu.VMEM((2, 2, span, columns), bf16),
            pltpu.VMEM((3, 2, span, columns), bf16),
            pltpu.VMEM((2, 2, span, kept), bf16),
            pltpu.VMEM((2, span, kept), bf16),
            pltpu.VMEM((3, FAR_DILATION, steps, columns), bf16),
            pltpu.VMEM((3, classes, n, steps, columns), bf16),
            pltpu.VMEM((classes, n, steps, columns), bf16),
            pltpu.VMEM((classes, n, steps, columns), bf16),
            pltpu.VMEM((classes, n, 1, 128), jnp.float32),
            pltpu.VMEM((classes, n, 1, 128), jnp.float32),
            pltpu.VMEM((m, length, columns), bf16),
            pltpu.VMEM((out_weight.shape[1] // 128, length, 128), jnp.float32),
            dma((7,)),
            dma((9,)),
            dma((1 + 2 * classes,)),
            dma((2,)),
            dma((2,)),
            dma((3,)),
            dma((3,)),
            dma((2,)),
            dma((2,)),
            dma((2,)),
            dma((2,)),
            dma((3, n)),
            dma((3, n)),
            dma((classes, n)),
            dma((classes, n)),
            dma((classes, n)),
            dma((classes, n)),
            dma((2, m)),
            dma((2, m)),
        ],
        compiler_params=pltpu.CompilerParams(
            collective_id=0, has_side_effects=True, vmem_limit_bytes=60 * 1024 * 1024
        ),
    )(tokens, query_weight, key_weight, value_weight, out_weight, jnp.asarray(table), jnp.asarray(base))


def planned(n, m, *arrays):
    length, columns = arrays[0].shape[0], arrays[1].shape[2]
    fits = (
        n == 8
        and m % 2 == 0
        and FAR_DILATION == 2 * n
        and MIDDLE_DILATION == 4
        and length == SIDE_STEPS * MIDDLE_DILATION
        and length % (FAR_DILATION * 16) == 0
        and columns % 128 == 0
        and arrays[4].shape[1] % 128 == 0
        and 3 * (columns // HEAD_DIM) <= 128
        and columns // HEAD_DIM * (length // FAR_DILATION) <= 128
    )
    if fits:
        return fused(n, m, *arrays)
    return per_device(*arrays)


def solution(mesh):
    placed = (
        P("sp", None),
        P(None, None, "tp"),
        P(None, None, "tp"),
        P(None, None, "tp"),
        P(None, "tp"),
    )
    return jax.shard_map(
        functools.partial(planned, mesh.shape["sp"], mesh.shape["tp"]),
        mesh=mesh,
        in_specs=placed,
        out_specs=P("sp", "tp"),
        check_vma=False,
    )
```

```python
import functools
import math

import jax
import numpy as np
import jax.numpy as jnp
from jax import lax
from jax.experimental import pallas as pl
from jax.experimental.pallas import tpu as pltpu
from jax.sharding import PartitionSpec as P

HEAD_DIM = 64
SIDE_STEPS = 64
MIDDLE_DILATION = 4
FAR_DILATION = 16
MESH = pl.DeviceIdType.MESH


def shifted(block, axis, distance):
    devices = range(lax.axis_size(axis))
    route = [(i - distance, i) for i in devices if i - distance in devices]
    return lax.ppermute(block, axis, route)


def with_halo(block, sides, width):
    for axis, dim in sides:
        count = lax.axis_size(axis)
        forward = [(i, i + 1) for i in range(count - 1)]
        backward = [(target, source) for source, target in forward]
        low = lax.ppermute(
            lax.slice_in_dim(block, block.shape[dim] - width, None, axis=dim), axis, forward
        )
        high = lax.ppermute(lax.slice_in_dim(block, 0, width, axis=dim), axis, backward)
        block = jnp.concatenate([low, block, high], axis=dim)
    return block


def rotate(projected, offset_pos):
    length, columns = projected.shape
    heads = columns // HEAD_DIM
    half = HEAD_DIM // 2
    positions = (offset_pos + jnp.arange(length)).astype(jnp.float32)
    inverse = 1.0 / 10000.0 ** (jnp.arange(half, dtype=jnp.float32) * 2.0 / HEAD_DIM)
    angles = positions[:, None] * inverse[None, :]
    angles = jnp.concatenate([angles, angles], axis=-1)
    cosine_table = jnp.cos(angles)[:, None, :]
    sine = jnp.sin(angles)[:, None, :]
    shaped = projected.reshape(length, heads, HEAD_DIM)
    turned = jnp.concatenate([-shaped[..., half:], shaped[..., :half]], axis=-1)
    return (shaped * cosine_table + turned * sine).reshape(length, columns)


def banded(queries, key_ext, value_ext, dilation, offset_pos, seq_len):
    length, columns = queries.shape
    heads = columns // HEAD_DIM
    class_len = length // dilation
    block_len = math.gcd(SIDE_STEPS, class_len)
    blocks = class_len // block_len
    extra = 2 * SIDE_STEPS // block_len
    query_blocks = queries.reshape(blocks, block_len, dilation, heads, HEAD_DIM)
    key_blocks = key_ext.reshape(blocks + extra, block_len, dilation, heads, HEAD_DIM)
    value_blocks = value_ext.reshape(blocks + extra, block_len, dilation, heads, HEAD_DIM)
    key_win = jnp.concatenate(
        [key_blocks[shift_idx : shift_idx + blocks] for shift_idx in range(extra + 1)], axis=1
    )
    value_win = jnp.concatenate(
        [value_blocks[shift_idx : shift_idx + blocks] for shift_idx in range(extra + 1)], axis=1
    )
    scores = jnp.einsum(
        "bqrhe,bkrhe->brhqk", query_blocks, key_win, preferred_element_type=jnp.float32
    )
    scores = scores * HEAD_DIM ** (-0.5)
    width_keys = key_win.shape[1]
    relative = jnp.arange(width_keys)[None, :] - jnp.arange(block_len)[:, None]
    within = (relative >= 0) & (relative <= 2 * SIDE_STEPS)
    key_rows = jnp.arange(blocks)[:, None] * block_len + jnp.arange(width_keys)[None, :]
    spots = (
        offset_pos
        - SIDE_STEPS * dilation
        + dilation * key_rows[:, :, None]
        + jnp.arange(dilation)[None, None, :]
    )
    inside = (spots >= 0) & (spots < seq_len)
    allowed = within[None, None, None] & jnp.transpose(inside, (0, 2, 1))[:, :, None, None, :]
    scores = jnp.where(allowed, scores, -1e30)
    row_max = jnp.max(scores, axis=-1, keepdims=True)
    expo = jnp.exp(scores - row_max)
    denom = jnp.sum(expo, axis=-1)
    probs = expo.astype(jnp.bfloat16)
    summed = jnp.einsum("brhqk,bkrhe->bqrhe", probs, value_win, preferred_element_type=jnp.float32)
    group_out = summed / jnp.transpose(denom, (0, 3, 1, 2))[..., None]
    log_sum = row_max[..., 0] + jnp.log(denom)
    log_sum = jnp.transpose(log_sum, (0, 3, 1, 2)).reshape(length, heads)
    return (group_out.reshape(length, columns), log_sum)


def collect(own_block, needed, direction):
    collected = own_block[None]
    while collected.shape[0] < needed + 1:
        stride = collected.shape[0]
        to_send = min(stride, needed + 1 - stride)
        arrived = shifted(collected[:to_send], "sp", direction * stride)
        collected = jnp.concatenate([collected, arrived], axis=0)
    return collected[1:]


def per_device(tokens, query_weight, key_weight, value_weight, out_weight):
    length = tokens.shape[0]
    offset_pos = lax.axis_index("sp") * length
    seq_len = lax.axis_size("sp") * length
    group_dilations = (1, MIDDLE_DILATION, FAR_DILATION)
    query_list = []
    pairs = []
    for group_idx in range(3):
        queries = rotate(
            jnp.dot(tokens, query_weight[group_idx], preferred_element_type=jnp.float32), offset_pos
        )
        keys_here = rotate(
            jnp.dot(tokens, key_weight[group_idx], preferred_element_type=jnp.float32), offset_pos
        )
        values_here = jnp.dot(tokens, value_weight[group_idx], preferred_element_type=jnp.float32)
        query_list.append(queries.astype(jnp.bfloat16))
        pairs.append(
            jnp.stack([keys_here.astype(jnp.bfloat16), values_here.astype(jnp.bfloat16)], axis=0)
        )
    middle_span_length = SIDE_STEPS * MIDDLE_DILATION
    first_ext = with_halo(pairs[0], (("sp", 1),), SIDE_STEPS)
    middle_ext = with_halo(pairs[1], (("sp", 1),), middle_span_length)
    far_span_length = SIDE_STEPS * FAR_DILATION
    needed = -(-far_span_length // length)
    lower_blocks = collect(pairs[2], needed, 1)
    upper_blocks = collect(pairs[2], needed, -1)
    columns = pairs[2].shape[2]
    lower_flat = jnp.moveaxis(lower_blocks[::-1], 0, 1).reshape(2, needed * length, columns)
    upper_flat = jnp.moveaxis(upper_blocks, 0, 1).reshape(2, needed * length, columns)
    far_full = jnp.concatenate([lower_flat, pairs[2], upper_flat], axis=1)
    extended = (first_ext, middle_ext, far_full)
    outputs = []
    log_sums = []
    for group_idx in range(3):
        group_out, log_sum = banded(
            query_list[group_idx],
            extended[group_idx][0],
            extended[group_idx][1],
            group_dilations[group_idx],
            offset_pos,
            seq_len,
        )
        outputs.append(group_out)
        log_sums.append(log_sum)
    merge_w = jax.nn.softmax(jnp.stack(log_sums, axis=0), axis=0)
    heads = columns // HEAD_DIM
    stacked = jnp.stack(outputs, axis=0).reshape(3, length, heads, HEAD_DIM)
    merged = (
        jnp.sum(merge_w[..., None] * stacked, axis=0).reshape(length, columns).astype(jnp.bfloat16)
    )
    mixed = jnp.dot(
        lax.all_gather(merged, "tp", axis=1, tiled=True),
        out_weight,
        preferred_element_type=jnp.float32,
    )
    return mixed.astype(jnp.bfloat16)


def remote(src, dst, send_sem, recv_sem, axis, target):
    return pltpu.make_async_remote_copy(
        src_ref=src,
        dst_ref=dst,
        send_sem=send_sem,
        recv_sem=recv_sem,
        device_id={axis: target},
        device_id_type=MESH,
    )


def head_mask(columns, head):
    lane = lax.broadcasted_iota(jnp.int32, (1, columns), 1)
    return (lane // HEAD_DIM == head).astype(jnp.float32)


def attend(queries, keys, values, bias):
    rows, columns = queries.shape
    heads = columns // HEAD_DIM
    masks = [head_mask(columns, head) for head in range(heads)]
    stacked = jnp.concatenate([queries * mask.astype(jnp.bfloat16) for mask in masks], axis=0)
    scores = lax.dot_general(
        stacked, keys, (((1,), (1,)), ((), ())), preferred_element_type=jnp.float32
    )
    width = keys.shape[0]
    scores = (scores.reshape(heads, rows, width) + bias[None]).reshape(heads * rows, width)
    row_max = jnp.max(scores, axis=-1, keepdims=True)
    expo = jnp.exp(scores - row_max)
    denom = jnp.sum(expo, axis=-1, keepdims=True)
    summed = jnp.dot(expo.astype(jnp.bfloat16), values, preferred_element_type=jnp.float32)
    summed = summed / denom
    lse = row_max + jnp.log(denom)
    parts = [slice(head * rows, (head + 1) * rows) for head in range(heads)]
    out = sum(summed[part] * mask for part, mask in zip(parts, masks))
    return out, [lse[part] for part in parts]


def in_terms(block):
    terms = []
    for _ in range(3):
        rounded = block.astype(jnp.bfloat16)
        terms.append(rounded)
        block = block - rounded.astype(jnp.float32)
    return jnp.concatenate(terms, axis=1)


def band_bias(rows, width, offset, low, high, stride=1):
    query = lax.broadcasted_iota(jnp.int32, (rows, width), 0)
    key = lax.broadcasted_iota(jnp.int32, (rows, width), 1)
    query = (query % (rows // stride)) * stride + query // (rows // stride)
    step = key + offset - query
    keep = (step >= -SIDE_STEPS) & (step <= SIDE_STEPS) & (key >= low) & (key < high)
    return jnp.where(keep, 0.0, -1e30)


def one_hot(size, source_of_row):
    row = lax.broadcasted_iota(jnp.int32, (size, size), 0)
    column = lax.broadcasted_iota(jnp.int32, (size, size), 1)
    return (source_of_row(row) == column).astype(jnp.float32).astype(jnp.bfloat16)


def scope(name):
    return jax.named_scope(name)


def take(ref, sem):
    pltpu.make_async_copy(ref, ref, sem).wait()


def fused_kernel(
    n, m, tokens_hbm, query_hbm, key_hbm, value_hbm, out_hbm, table_hbm, result_ref,
    tokens, weights, out_weight, table, kv_first, mid_kv, mid_q, mid_send, mid_ret, mid_back,
    mid_lse, mid_lse_back, far_send, far_recv, back_send, back_recv, lse_send, lse_recv,
    merged_all, result_wide, load_sem, weight_sem, first_sem, pair_sem, hop_sem, ret_sem,
    far_sem, back_sem, tp_send_sem, tp_recv_sem,
):
    me = lax.axis_index("sp")
    mine = lax.axis_index("tp")
    side = lax.rem(me, 2)
    partner = me + 1 - 2 * side
    length, columns = tokens.shape[0], weights.shape[-1]
    depth = tokens.shape[1]
    heads = columns // HEAD_DIM
    half = HEAD_DIM // 2
    classes = FAR_DILATION // n
    far_steps = length // FAR_DILATION
    halo = SIDE_STEPS
    steps = length // MIDDLE_DILATION
    piece = length // 2
    sub = steps // 8

    table_load = pltpu.make_async_copy(table_hbm, table, load_sem.at[0])
    table_load.start()
    chunks = 4
    chunk = depth // chunks
    for index in range(chunks):
        part = pl.ds(index * chunk, chunk)
        sem = load_sem.at[1 + index]
        pltpu.make_async_copy(tokens_hbm.at[:, part], tokens.at[:, part], sem).start()
        pltpu.make_async_copy(key_hbm.at[2, part], weights.at[7, part], sem).start()
    out_load = pltpu.make_async_copy(out_hbm, out_weight, load_sem.at[1 + chunks])
    sources = (query_hbm, key_hbm, value_hbm)
    order = ((2, 2), (2, 0), (1, 1), (1, 2), (1, 0), (0, 1), (0, 2), (0, 0))
    waiting = []
    weight_loads = {}
    for index, (group, kind) in enumerate(order):
        slot = group * 3 + kind
        load = pltpu.make_async_copy(
            sources[kind].at[group], weights.at[slot], weight_sem.at[index % 4]
        )
        weight_loads[group, kind] = load
        waiting.append(load)
    waiting.append(out_load)
    waiting.pop(0).start()

    barrier = pltpu.get_barrier_semaphore()
    for distance in range(1, n):
        pl.semaphore_signal(
            barrier, inc=1, device_id={"sp": lax.rem(me + distance, n)}, device_id_type=MESH
        )
    for distance in range(1, m):
        pl.semaphore_signal(
            barrier, inc=1, device_id={"tp": lax.rem(mine + distance, m)}, device_id_type=MESH
        )

    far_order = one_hot(
        length, lambda row: (row % far_steps) * FAR_DILATION + row // far_steps
    )
    middle_order = one_hot(
        length,
        lambda row: (row % steps) * MIDDLE_DILATION + (row // steps + 2 * side) % MIDDLE_DILATION,
    )
    tile = 2 * halo
    first_order = one_hot(
        length, lambda row: row // tile * tile + (row % halo) * 2 + row % tile // halo
    )
    lane = lax.broadcasted_iota(jnp.int32, (1, columns), 1)
    first_half = lane % HEAD_DIM < half

    def product_of(slot, low, size):
        return jnp.dot(
            tokens[:, low : low + size],
            weights[slot, low : low + size],
            preferred_element_type=jnp.float32,
        )

    def rolled(block, shift):
        return jnp.concatenate(
            [pltpu.roll(block[:, at : at + 128], shift, 1) for at in range(0, columns, 128)], axis=1
        )

    def turned(product, kind):
        if kind < 2:
            later = rolled(product, 128 - half)
            earlier = rolled(product, half)
            product = product * cosine + jnp.where(first_half, later, earlier) * sine
        if kind == 0:
            product = product * HEAD_DIM ** (-0.5)
        return product.astype(jnp.bfloat16)

    def project(group, kind):
        slot = group * 3 + kind
        weight_loads[group, kind].wait()
        if waiting:
            waiting.pop(0).start()
        return turned(product_of(slot, 0, depth), kind)

    def ordered(order, block):
        return jnp.dot(order, block, preferred_element_type=jnp.float32).astype(jnp.bfloat16)

    with scope("w_table"):
        table_load.wait()
    base_cos = table[0, pl.ds(length + me, 1), :]
    base_sin = table[1, pl.ds(length + me, 1), :]
    inner_cos = table[0, 0:length]
    inner_sin = table[1, 0:length]
    cosine = base_cos * inner_cos - base_sin * inner_sin
    sine = base_sin * inner_cos + base_cos * inner_sin
    wide = columns // cosine.shape[1]
    cosine = jnp.concatenate([cosine] * wide, axis=1)
    sine = jnp.concatenate([sine] * wide, axis=1) * jnp.where(first_half, -1.0, 1.0)
    first_product = None
    for index in range(chunks):
        with scope(f"w_load{index}"):
            take(weights.at[7, pl.ds(0, 2 * chunk)], load_sem.at[1 + index])
        term = product_of(7, index * chunk, chunk)
        first_product = term if first_product is None else first_product + term
    for _ in range(3):
        waiting.pop(0).start()

    def far(kind):
        with scope(f"p_far{kind}"):
            block = turned(first_product, 1) if kind == 1 else project(2, kind)
            far_send[kind] = ordered(far_order, block).reshape(far_send.shape[1:])
        if kind == 1:
            with scope("w_barrier"):
                pl.semaphore_wait(barrier, n - 1 + m - 1)
        for distance in range(1, n):
            target = lax.rem(me + distance, n)
            remote(
                far_send.at[kind, pl.ds(target * classes, classes)],
                far_recv.at[kind, :, me], far_sem.at[0], far_sem.at[1], "sp", target,
            ).start()
        pltpu.make_async_copy(
            far_send.at[kind, pl.ds(me * classes, classes)], far_recv.at[kind, :, me],
            far_sem.at[1],
        ).start()

    def middle(kind):
        with scope(f"p_mid{kind}"):
            block = ordered(middle_order, project(1, kind)).reshape(2, 2, steps, columns)
            if kind == 0:
                mid_q[:, pl.ds(side, 1)] = block[0][:, None]
                landing = mid_q.at[:, side]
            else:
                mid_kv[kind - 1, :, pl.ds(1 + side, 1)] = block[0][:, None]
                landing = mid_kv.at[kind - 1, :, 1 + side]
            mid_send[kind] = block[1]
        remote(
            mid_send.at[kind], landing, pair_sem.at[0], pair_sem.at[1 if kind else 2],
            "sp", partner,
        ).start()

    lean = 2 * side - 1
    has_ahead = (me + 2 * lean >= 0) & (me + 2 * lean < n)
    has_behind = (me - 2 * lean >= 0) & (me - 2 * lean < n)
    direct = remote(
        mid_kv.at[:, :, 1 + side], mid_kv.at[:, :, 3 * (1 - side)],
        hop_sem.at[0], hop_sem.at[1], "sp", lax.rem(me + 2 * lean + n, n),
    )
    relay = remote(
        mid_kv.at[:, :, 2 - side], mid_kv.at[:, :, 3 * side],
        hop_sem.at[2], hop_sem.at[3], "sp", lax.rem(me - 2 * lean + n, n),
    )

    far(1)
    far(2)
    far(0)
    middle(1)
    middle(2)

    @pl.when(has_ahead)
    def _():
        direct.start()

    middle(0)

    for kind in (1, 2):
        with scope(f"p_first{kind}"):
            kv_first[kind - 1, halo : halo + length] = project(0, kind)

    first_up = remote(
        kv_first.at[:, pl.ds(length, halo)], kv_first.at[:, pl.ds(0, halo)],
        first_sem.at[0], first_sem.at[1], "sp", lax.rem(me + 1, n),
    )
    first_down = remote(
        kv_first.at[:, pl.ds(halo, halo)], kv_first.at[:, pl.ds(halo + length, halo)],
        first_sem.at[2], first_sem.at[3], "sp", lax.rem(me + n - 1, n),
    )

    @pl.when(me < n - 1)
    def _():
        first_up.start()

    @pl.when(me > 0)
    def _():
        first_down.start()

    @pl.when(me == 0)
    def _():
        kv_first[:, :halo] = jnp.zeros((2, halo, columns), jnp.bfloat16)

    @pl.when(me == n - 1)
    def _():
        kv_first[:, halo + length :] = jnp.zeros((2, halo, columns), jnp.bfloat16)

    @pl.when(me < 2)
    def _():
        mid_kv[:, :, 0] = jnp.zeros_like(mid_kv[:, :, 0])

    @pl.when(me >= n - 2)
    def _():
        mid_kv[:, :, 3] = jnp.zeros_like(mid_kv[:, :, 3])

    with scope("p_first0"):
        first_queries = ordered(first_order, project(0, 0))

    with scope("w_pair"):
        take(mid_kv.at[:, :, 2 - side], pair_sem.at[1])

    @pl.when(has_behind)
    def _():
        relay.start()

    with scope("w_far"):
        take(far_recv, far_sem.at[1])
    class_len = n * far_steps
    far_bias = band_bias(class_len, class_len, 0, 0, class_len)
    row16 = lax.broadcasted_iota(jnp.int32, (class_len, 128), 0) % far_steps
    lane16 = lax.broadcasted_iota(jnp.int32, (class_len, 128), 1)
    diagonal = lane16 % far_steps == row16
    for index in range(classes):
        with scope(f"c_far{index}"):
            queries, keys, values = (
                far_recv[kind, index].reshape(class_len, columns) for kind in range(3)
            )
            out, lses = attend(queries, keys, values, far_bias)
            back_send[index] = out.astype(jnp.bfloat16).reshape(n, far_steps, columns)
            spread = sum(
                jnp.where(diagonal & (lane16 // far_steps == head), lse, 0.0)
                for head, lse in enumerate(lses)
            )
            lse_send[index] = jnp.sum(spread.reshape(n, far_steps, 128), axis=1, keepdims=True)
        for which, (source, landing) in enumerate(((back_send, back_recv), (lse_send, lse_recv))):
            for distance in range(1, n):
                target = lax.rem(me + distance, n)
                remote(
                    source.at[index, target], landing.at[index, me],
                    back_sem.at[which], back_sem.at[2 + 2 * index + which], "sp", target,
                ).start()
            pltpu.make_async_copy(
                source.at[index, me], landing.at[index, me], back_sem.at[2 + 2 * index + which]
            ).start()

    with scope("w_hop"):
        take(mid_q.at[:, 1 - side], pair_sem.at[2])

        @pl.when(has_ahead)
        def _():
            direct.wait_send()
            relay.wait_recv()

        @pl.when(has_behind)
        def _():
            relay.wait_send()
            direct.wait_recv()

    low = jnp.where(me < 2, steps, 0)
    high = jnp.where(me >= n - 2, 3 * steps, 4 * steps)
    middle_bias = band_bias(2 * steps, 4 * steps, -steps, low, high)
    sub_row = lax.broadcasted_iota(jnp.int32, (2 * steps, 128), 0) % steps // 8
    sub_lane = lax.broadcasted_iota(jnp.int32, (2 * steps, 128), 1)
    for index in range(2):
        with scope(f"c_mid{index}"):
            out, lses = attend(
                mid_q[index].reshape(2 * steps, columns),
                mid_kv[0, index].reshape(4 * steps, columns),
                mid_kv[1, index].reshape(4 * steps, columns),
                middle_bias,
            )
            mid_ret[index] = out.astype(jnp.bfloat16).reshape(2, steps, columns)
            spread = sum(
                jnp.where((sub_lane % sub == sub_row) & (sub_lane // sub == head), lse, 0.0)
                for head, lse in enumerate(lses)
            )
            mid_lse[index] = jnp.sum(spread.reshape(2, sub, 8, 128), axis=1)
        for which, (source, landing) in enumerate(((mid_ret, mid_back), (mid_lse, mid_lse_back))):
            remote(
                source.at[index, 1 - side], landing.at[index],
                ret_sem.at[which], ret_sem.at[2 + 2 * index + which], "sp", partner,
            ).start()

    with scope("w_first"):
        @pl.when(me < n - 1)
        def _():
            first_up.wait_send()
            first_down.wait_recv()

        @pl.when(me > 0)
        def _():
            first_down.wait_send()
            first_up.wait_recv()

    first_outs = []
    first_lses = []
    with scope("c_first"):
        for start in range(0, length, tile):
            width = tile + 2 * halo
            low = halo - start - me * length
            high = halo - start + (n - me) * length
            out, lses = attend(
                first_queries[start : start + tile],
                kv_first[0, start : start + width],
                kv_first[1, start : start + width],
                band_bias(tile, width, -halo, low, high, 2),
            )
            first_outs.append(out)
            first_lses.append(
                sum(lse * head_mask(columns, head) for head, lse in enumerate(lses))
            )

    def lane_spread(group):
        term = lax.broadcasted_iota(jnp.int32, (128, columns), 0)
        column = lax.broadcasted_iota(jnp.int32, (128, columns), 1)
        keep = (term // group == column // HEAD_DIM).astype(jnp.float32).astype(jnp.bfloat16)
        return jnp.concatenate([keep] * 3, axis=0)

    middle_spread = lane_spread(sub)
    far_spread = lane_spread(far_steps)
    middle_natural = one_hot(
        piece, lambda row: row // 2 + steps * ((row % 2 + side) % 2)
    )
    far_natural = one_hot(piece, lambda row: (row % n) * far_steps + row // n)
    position = lax.broadcasted_iota(jnp.int32, (piece, 128), 0) // n
    lane_part = lax.broadcasted_iota(jnp.int32, (piece, 128), 1)
    far_keep = (lane_part % far_steps == position) & (lane_part < heads * far_steps)
    middle_keep = (sub_lane % sub == sub_row) & (sub_lane < heads * sub)

    near = []
    for part in range(2):
        with scope(f"w_ret{part}"):
            take(mid_back.at[part], ret_sem.at[2 + 2 * part])
            take(mid_lse_back.at[part], ret_sem.at[3 + 2 * part])
        with scope(f"c_near{part}"):
            block = jnp.concatenate([mid_ret[part, side], mid_back[part]], axis=0)
            block = jnp.dot(middle_natural, block, preferred_element_type=jnp.float32)
            lse = jnp.concatenate(
                [mid_lse[part, side]] * sub + [mid_lse_back[part]] * sub, axis=0
            )
            lse = in_terms(jnp.where(middle_keep, lse, 0.0))
            lse = jnp.dot(middle_natural, lse, preferred_element_type=jnp.float32)
            middle_lse = jnp.dot(
                lse.astype(jnp.bfloat16), middle_spread, preferred_element_type=jnp.float32
            )
            rows = slice(part * halo, (part + 1) * halo)
            first_out = jnp.concatenate([out[rows] for out in first_outs], axis=0)
            first_lse = jnp.concatenate([lse[rows] for lse in first_lses], axis=0)
            top = jnp.maximum(first_lse, middle_lse)
            first_w = jnp.exp(first_lse - top)
            middle_w = jnp.exp(middle_lse - top)
            near.append((first_w * first_out + middle_w * block, first_w + middle_w, top))

    chips = m // 2
    sibling = mine + 1 - 2 * lax.rem(mine, 2)

    def hand(part, source, slot, target):
        rows = pl.ds(part * piece, piece)
        copy = remote(
            merged_all.at[source, rows], merged_all.at[slot, rows],
            tp_send_sem.at[0], tp_recv_sem.at[part, slot - 1], "tp", target,
        )
        copy.start()
        return copy

    def term(part, slot):
        chip = slot % chips
        owner = lax.rem((mine if slot < chips else sibling) - 2 * chip + m, m)
        rows = pl.ds(pl.multiple_of(owner * columns, columns), columns)
        return jnp.dot(
            merged_all[slot, part * piece : (part + 1) * piece],
            out_weight[rows, :],
            preferred_element_type=jnp.float32,
        )

    copies = {}
    totals = []
    with scope("w_outw"):
        out_load.wait()
    for part in range(2):
        with scope(f"w_back{part}"):
            take(back_recv.at[part], back_sem.at[2 + 2 * part])
            take(lse_recv.at[part], back_sem.at[3 + 2 * part])
        with scope(f"c_merge{part}"):
            far_out = jnp.dot(
                far_natural,
                back_recv[part].reshape(piece, columns),
                preferred_element_type=jnp.float32,
            )
            lse = jnp.concatenate([lse_recv[part].reshape(n, 128)] * (piece // n), axis=0)
            lse = jnp.where(far_keep, lse, 0.0)
            far_lse = jnp.dot(in_terms(lse), far_spread, preferred_element_type=jnp.float32)
            total, weight, near_top = near[part]
            top = jnp.maximum(near_top, far_lse)
            near_w = jnp.exp(near_top - top)
            far_w = jnp.exp(far_lse - top)
            merged = (near_w * total + far_w * far_out) / (near_w * weight + far_w)
            merged_all[0, part * piece : (part + 1) * piece] = merged.astype(jnp.bfloat16)
        for chip in range(1, chips):
            copies[part, chip] = hand(part, 0, chip, lax.rem(mine + 2 * chip, m))
        copies[part, chips] = hand(part, 0, chips, sibling)
        totals.append(term(part, 0))

    take(mid_send, pair_sem.at[0])
    take(far_send.at[:, pl.ds(0, FAR_DILATION - classes)], far_sem.at[0])
    take(back_send.at[:, pl.ds(0, n - 1)], back_sem.at[0])
    take(lse_send.at[:, pl.ds(0, n - 1)], back_sem.at[1])
    take(mid_back, ret_sem.at[0])
    take(mid_lse_back, ret_sem.at[1])

    for part in range(2):
        for chip in range(1, chips):
            with scope(f"w_chip{part}"):
                copies[part, chip].wait_recv()
            copies[part, chips + chip] = hand(part, chip, chips + chip, sibling)
        with scope(f"w_sib{part}"):
            copies[part, chips].wait_recv()
        totals[part] = totals[part] + term(part, chips)
        for chip in range(1, chips):
            totals[part] = totals[part] + term(part, chip)
    for part in range(2):
        for chip in range(1, chips):
            with scope(f"w_fwd{part}"):
                copies[part, chips + chip].wait_recv()
            totals[part] = totals[part] + term(part, chips + chip)
        for index in range(result_wide.shape[0]):
            result_wide[index, pl.ds(part, piece, stride=2), :] = totals[part][
                :, index * 128 : (index + 1) * 128
            ]
    for index in range(result_wide.shape[0]):
        result_ref[:, index * 128 : (index + 1) * 128] = result_wide[index].astype(
            result_ref.dtype
        )
    take(merged_all.at[pl.ds(1, m - 1)], tp_send_sem.at[0])


def turn_tables(n, length):
    half = HEAD_DIM // 2
    inverse = 1.0 / 10000.0 ** (np.arange(half, dtype=np.float32) * np.float32(2.0) / HEAD_DIM)
    inverse = np.tile(inverse.astype(np.float64), 128 // half)[None]
    positions = np.concatenate([np.arange(length), np.arange(n) * length])
    angles = positions[:, None] * inverse
    return np.stack([np.cos(angles), np.sin(angles)]).astype(np.float32)


def fused(n, m, tokens, query_weight, key_weight, value_weight, out_weight):
    length, width = tokens.shape
    columns = query_weight.shape[2]
    table = turn_tables(n, length)
    steps = length // FAR_DILATION
    span = length // MIDDLE_DILATION
    classes = FAR_DILATION // n
    bf16 = jnp.bfloat16
    hbm = pl.BlockSpec(memory_space=pl.ANY)
    vmem = pl.BlockSpec(memory_space=pltpu.VMEM)
    dma = pltpu.SemaphoreType.DMA
    return pl.pallas_call(
        functools.partial(fused_kernel, n, m),
        out_shape=pltpu.VMEM((length, out_weight.shape[1]), bf16),
        in_specs=[hbm] * 6,
        out_specs=vmem,
        scratch_shapes=[
            pltpu.VMEM((length, width), bf16),
            pltpu.VMEM((9, width, columns), bf16),
            pltpu.VMEM(out_weight.shape, bf16),
            pltpu.VMEM(table.shape, jnp.float32),
            pltpu.VMEM((2, length + 2 * SIDE_STEPS, columns), bf16),
            pltpu.VMEM((2, 2, 4, span, columns), bf16),
            pltpu.VMEM((2, 2, span, columns), bf16),
            pltpu.VMEM((3, 2, span, columns), bf16),
            pltpu.VMEM((2, 2, span, columns), bf16),
            pltpu.VMEM((2, span, columns), bf16),
            pltpu.VMEM((2, 2, 8, 128), jnp.float32),
            pltpu.VMEM((2, 8, 128), jnp.float32),
            pltpu.VMEM((3, FAR_DILATION, steps, columns), bf16),
            pltpu.VMEM((3, classes, n, steps, columns), bf16),
            pltpu.VMEM((classes, n, steps, columns), bf16),
            pltpu.VMEM((classes, n, steps, columns), bf16),
            pltpu.VMEM((classes, n, 1, 128), jnp.float32),
            pltpu.VMEM((classes, n, 1, 128), jnp.float32),
            pltpu.VMEM((m, length, columns), bf16),
            pltpu.VMEM((out_weight.shape[1] // 128, length, 128), jnp.float32),
            dma((6,)),
            dma((4,)),
            dma((4,)),
            dma((3,)),
            dma((4,)),
            dma((6,)),
            dma((2,)),
            dma((2 + 2 * classes,)),
            dma((1,)),
            dma((2, m - 1)),
        ],
        compiler_params=pltpu.CompilerParams(
            collective_id=0, has_side_effects=True, vmem_limit_bytes=60 * 1024 * 1024
        ),
    )(tokens, query_weight, key_weight, value_weight, out_weight, jnp.asarray(table))


def planned(n, m, *arrays):
    length, columns = arrays[0].shape[0], arrays[1].shape[2]
    fits = (
        n == 8
        and m % 2 == 0
        and FAR_DILATION == 2 * n
        and MIDDLE_DILATION == 4
        and length == SIDE_STEPS * MIDDLE_DILATION
        and length % (FAR_DILATION * 16) == 0
        and columns % 128 == 0
        and arrays[4].shape[1] % 128 == 0
        and 3 * (columns // HEAD_DIM) <= 128
        and columns // HEAD_DIM * (length // FAR_DILATION) <= 128
    )
    if fits:
        return fused(n, m, *arrays)
    return per_device(*arrays)


def solution(mesh):
    placed = (
        P("sp", None),
        P(None, None, "tp"),
        P(None, None, "tp"),
        P(None, None, "tp"),
        P(None, "tp"),
    )
    return jax.shard_map(
        functools.partial(planned, mesh.shape["sp"], mesh.shape["tp"]),
        mesh=mesh,
        in_specs=placed,
        out_specs=P("sp", "tp"),
        check_vma=False,
    )
```

```python
import functools
import math

import jax
import numpy as np
import jax.numpy as jnp
from jax import lax
from jax.experimental import pallas as pl
from jax.experimental.pallas import tpu as pltpu
from jax.sharding import PartitionSpec as P

HEAD_DIM = 64
SIDE_STEPS = 64
MIDDLE_DILATION = 4
FAR_DILATION = 16
MESH = pl.DeviceIdType.MESH


def shifted(block, axis, distance):
    devices = range(lax.axis_size(axis))
    route = [(i - distance, i) for i in devices if i - distance in devices]
    return lax.ppermute(block, axis, route)


def with_halo(block, sides, width):
    for axis, dim in sides:
        count = lax.axis_size(axis)
        forward = [(i, i + 1) for i in range(count - 1)]
        backward = [(target, source) for source, target in forward]
        low = lax.ppermute(
            lax.slice_in_dim(block, block.shape[dim] - width, None, axis=dim), axis, forward
        )
        high = lax.ppermute(lax.slice_in_dim(block, 0, width, axis=dim), axis, backward)
        block = jnp.concatenate([low, block, high], axis=dim)
    return block


def rotate(projected, offset_pos):
    length, columns = projected.shape
    heads = columns // HEAD_DIM
    half = HEAD_DIM // 2
    positions = (offset_pos + jnp.arange(length)).astype(jnp.float32)
    inverse = 1.0 / 10000.0 ** (jnp.arange(half, dtype=jnp.float32) * 2.0 / HEAD_DIM)
    angles = positions[:, None] * inverse[None, :]
    angles = jnp.concatenate([angles, angles], axis=-1)
    cosine_table = jnp.cos(angles)[:, None, :]
    sine = jnp.sin(angles)[:, None, :]
    shaped = projected.reshape(length, heads, HEAD_DIM)
    turned = jnp.concatenate([-shaped[..., half:], shaped[..., :half]], axis=-1)
    return (shaped * cosine_table + turned * sine).reshape(length, columns)


def banded(queries, key_ext, value_ext, dilation, offset_pos, seq_len):
    length, columns = queries.shape
    heads = columns // HEAD_DIM
    class_len = length // dilation
    block_len = math.gcd(SIDE_STEPS, class_len)
    blocks = class_len // block_len
    extra = 2 * SIDE_STEPS // block_len
    query_blocks = queries.reshape(blocks, block_len, dilation, heads, HEAD_DIM)
    key_blocks = key_ext.reshape(blocks + extra, block_len, dilation, heads, HEAD_DIM)
    value_blocks = value_ext.reshape(blocks + extra, block_len, dilation, heads, HEAD_DIM)
    key_win = jnp.concatenate(
        [key_blocks[shift_idx : shift_idx + blocks] for shift_idx in range(extra + 1)], axis=1
    )
    value_win = jnp.concatenate(
        [value_blocks[shift_idx : shift_idx + blocks] for shift_idx in range(extra + 1)], axis=1
    )
    scores = jnp.einsum(
        "bqrhe,bkrhe->brhqk", query_blocks, key_win, preferred_element_type=jnp.float32
    )
    scores = scores * HEAD_DIM ** (-0.5)
    width_keys = key_win.shape[1]
    relative = jnp.arange(width_keys)[None, :] - jnp.arange(block_len)[:, None]
    within = (relative >= 0) & (relative <= 2 * SIDE_STEPS)
    key_rows = jnp.arange(blocks)[:, None] * block_len + jnp.arange(width_keys)[None, :]
    spots = (
        offset_pos
        - SIDE_STEPS * dilation
        + dilation * key_rows[:, :, None]
        + jnp.arange(dilation)[None, None, :]
    )
    inside = (spots >= 0) & (spots < seq_len)
    allowed = within[None, None, None] & jnp.transpose(inside, (0, 2, 1))[:, :, None, None, :]
    scores = jnp.where(allowed, scores, -1e30)
    row_max = jnp.max(scores, axis=-1, keepdims=True)
    expo = jnp.exp(scores - row_max)
    denom = jnp.sum(expo, axis=-1)
    probs = expo.astype(jnp.bfloat16)
    summed = jnp.einsum("brhqk,bkrhe->bqrhe", probs, value_win, preferred_element_type=jnp.float32)
    group_out = summed / jnp.transpose(denom, (0, 3, 1, 2))[..., None]
    log_sum = row_max[..., 0] + jnp.log(denom)
    log_sum = jnp.transpose(log_sum, (0, 3, 1, 2)).reshape(length, heads)
    return (group_out.reshape(length, columns), log_sum)


def collect(own_block, needed, direction):
    collected = own_block[None]
    while collected.shape[0] < needed + 1:
        stride = collected.shape[0]
        to_send = min(stride, needed + 1 - stride)
        arrived = shifted(collected[:to_send], "sp", direction * stride)
        collected = jnp.concatenate([collected, arrived], axis=0)
    return collected[1:]


def per_device(tokens, query_weight, key_weight, value_weight, out_weight):
    length = tokens.shape[0]
    offset_pos = lax.axis_index("sp") * length
    seq_len = lax.axis_size("sp") * length
    group_dilations = (1, MIDDLE_DILATION, FAR_DILATION)
    query_list = []
    pairs = []
    for group_idx in range(3):
        queries = rotate(
            jnp.dot(tokens, query_weight[group_idx], preferred_element_type=jnp.float32), offset_pos
        )
        keys_here = rotate(
            jnp.dot(tokens, key_weight[group_idx], preferred_element_type=jnp.float32), offset_pos
        )
        values_here = jnp.dot(tokens, value_weight[group_idx], preferred_element_type=jnp.float32)
        query_list.append(queries.astype(jnp.bfloat16))
        pairs.append(
            jnp.stack([keys_here.astype(jnp.bfloat16), values_here.astype(jnp.bfloat16)], axis=0)
        )
    middle_span_length = SIDE_STEPS * MIDDLE_DILATION
    first_ext = with_halo(pairs[0], (("sp", 1),), SIDE_STEPS)
    middle_ext = with_halo(pairs[1], (("sp", 1),), middle_span_length)
    far_span_length = SIDE_STEPS * FAR_DILATION
    needed = -(-far_span_length // length)
    lower_blocks = collect(pairs[2], needed, 1)
    upper_blocks = collect(pairs[2], needed, -1)
    columns = pairs[2].shape[2]
    lower_flat = jnp.moveaxis(lower_blocks[::-1], 0, 1).reshape(2, needed * length, columns)
    upper_flat = jnp.moveaxis(upper_blocks, 0, 1).reshape(2, needed * length, columns)
    far_full = jnp.concatenate([lower_flat, pairs[2], upper_flat], axis=1)
    extended = (first_ext, middle_ext, far_full)
    outputs = []
    log_sums = []
    for group_idx in range(3):
        group_out, log_sum = banded(
            query_list[group_idx],
            extended[group_idx][0],
            extended[group_idx][1],
            group_dilations[group_idx],
            offset_pos,
            seq_len,
        )
        outputs.append(group_out)
        log_sums.append(log_sum)
    merge_w = jax.nn.softmax(jnp.stack(log_sums, axis=0), axis=0)
    heads = columns // HEAD_DIM
    stacked = jnp.stack(outputs, axis=0).reshape(3, length, heads, HEAD_DIM)
    merged = (
        jnp.sum(merge_w[..., None] * stacked, axis=0).reshape(length, columns).astype(jnp.bfloat16)
    )
    mixed = jnp.dot(
        lax.all_gather(merged, "tp", axis=1, tiled=True),
        out_weight,
        preferred_element_type=jnp.float32,
    )
    return mixed.astype(jnp.bfloat16)


def remote(src, dst, send_sem, recv_sem, axis, target):
    return pltpu.make_async_remote_copy(
        src_ref=src,
        dst_ref=dst,
        send_sem=send_sem,
        recv_sem=recv_sem,
        device_id={axis: target},
        device_id_type=MESH,
    )


def head_mask(columns, head):
    lane = lax.broadcasted_iota(jnp.int32, (1, columns), 1)
    return (lane // HEAD_DIM == head).astype(jnp.float32)


def attend(queries, keys, values, bias):
    rows, columns = queries.shape
    heads = columns // HEAD_DIM
    masks = [head_mask(columns, head) for head in range(heads)]
    stacked = jnp.concatenate([queries * mask.astype(jnp.bfloat16) for mask in masks], axis=0)
    scores = lax.dot_general(
        stacked, keys, (((1,), (1,)), ((), ())), preferred_element_type=jnp.float32
    )
    width = keys.shape[0]
    scores = (scores.reshape(heads, rows, width) + bias[None]).reshape(heads * rows, width)
    row_max = jnp.max(scores, axis=-1, keepdims=True)
    expo = jnp.exp(scores - row_max)
    denom = jnp.sum(expo, axis=-1, keepdims=True)
    summed = jnp.dot(expo.astype(jnp.bfloat16), values, preferred_element_type=jnp.float32)
    summed = summed / denom
    lse = row_max + jnp.log(denom)
    parts = [slice(head * rows, (head + 1) * rows) for head in range(heads)]
    out = sum(summed[part] * mask for part, mask in zip(parts, masks))
    return out, [lse[part] for part in parts]


def in_terms(block):
    terms = []
    for _ in range(3):
        rounded = block.astype(jnp.bfloat16)
        terms.append(rounded)
        block = block - rounded.astype(jnp.float32)
    return jnp.concatenate(terms, axis=1)


def band_bias(rows, width, offset, low, high, stride=1):
    query = lax.broadcasted_iota(jnp.int32, (rows, width), 0)
    key = lax.broadcasted_iota(jnp.int32, (rows, width), 1)
    query = (query % (rows // stride)) * stride + query // (rows // stride)
    step = key + offset - query
    keep = (step >= -SIDE_STEPS) & (step <= SIDE_STEPS) & (key >= low) & (key < high)
    return jnp.where(keep, 0.0, -1e30)


def one_hot(size, source_of_row):
    row = lax.broadcasted_iota(jnp.int32, (size, size), 0)
    column = lax.broadcasted_iota(jnp.int32, (size, size), 1)
    return (source_of_row(row) == column).astype(jnp.float32).astype(jnp.bfloat16)


def scope(name):
    return jax.named_scope(name)


def take(ref, sem):
    pltpu.make_async_copy(ref, ref, sem).wait()


def fused_kernel(
    n, m, tokens_hbm, query_hbm, key_hbm, value_hbm, out_hbm, table_hbm, result_ref,
    tokens, weights, out_weight, table, kv_first, mid_kv, mid_q, mid_send, mid_ret, mid_back,
    mid_lse, mid_lse_back, far_send, far_recv, back_send, back_recv, lse_send, lse_recv,
    merged_all, result_wide, natural, load_sem, first_sem, pair_sem, hop_sem, ret_sem,
    far_sem, back_sem, tp_send_sem, tp_recv_sem,
):
    me = lax.axis_index("sp")
    mine = lax.axis_index("tp")
    side = lax.rem(me, 2)
    partner = me + 1 - 2 * side
    length, columns = tokens.shape[0], weights.shape[-1]
    depth = tokens.shape[1]
    heads = columns // HEAD_DIM
    half = HEAD_DIM // 2
    classes = FAR_DILATION // n
    far_steps = length // FAR_DILATION
    halo = SIDE_STEPS
    steps = length // MIDDLE_DILATION
    piece = length // 2
    sub = steps // 8
    back_rows = n * (far_steps * columns // 256 + 1)
    ret_rows = steps * columns // 256 + 8

    table_load = pltpu.make_async_copy(table_hbm, table, load_sem.at[0])
    table_load.start()
    chunks = 4
    chunk = depth // chunks
    for index in range(chunks):
        part = pl.ds(index * chunk, chunk)
        sem = load_sem.at[1 + index]
        pltpu.make_async_copy(tokens_hbm.at[:, part], tokens.at[:, part], sem).start()
        pltpu.make_async_copy(key_hbm.at[2, part], weights.at[7, part], sem).start()
    out_load = pltpu.make_async_copy(out_hbm, out_weight, load_sem.at[2])
    sources = (query_hbm, key_hbm, value_hbm)
    order = ((2, 2), (2, 0), (1, 1), (1, 2), (1, 0), (0, 1), (0, 2), (0, 0))
    waiting = []
    weight_loads = {}
    for index, (group, kind) in enumerate(order):
        slot = group * 3 + kind
        load = pltpu.make_async_copy(
            sources[kind].at[group], weights.at[slot], load_sem.at[(5, 1, 2, 3, 4, 0, 5, 1)[index]]
        )
        weight_loads[group, kind] = load
        waiting.append(load)
    waiting.append(out_load)
    waiting.pop(0).start()

    barrier = pltpu.get_barrier_semaphore()
    for distance in range(1, n):
        pl.semaphore_signal(
            barrier, inc=1, device_id={"sp": lax.rem(me + distance, n)}, device_id_type=MESH
        )
    for distance in range(1, m):
        pl.semaphore_signal(
            barrier, inc=1, device_id={"tp": lax.rem(mine + distance, m)}, device_id_type=MESH
        )

    tile = 2 * halo
    lane = lax.broadcasted_iota(jnp.int32, (1, columns), 1)
    first_half = lane % HEAD_DIM < half

    def product_of(slot, low, size):
        return jnp.dot(
            tokens[:, low : low + size],
            weights[slot, low : low + size],
            preferred_element_type=jnp.float32,
        )

    def rolled(block, shift):
        return jnp.concatenate(
            [pltpu.roll(block[:, at : at + 128], shift, 1) for at in range(0, columns, 128)], axis=1
        )

    def turned(product, kind):
        if kind < 2:
            later = rolled(product, 128 - half)
            earlier = rolled(product, half)
            product = product * cosine + jnp.where(first_half, later, earlier) * sine
        if kind == 0:
            product = product * HEAD_DIM ** (-0.5)
        return product

    def project(group, kind):
        slot = group * 3 + kind
        weight_loads[group, kind].wait()
        if waiting:
            waiting.pop(0).start()
        return turned(product_of(slot, 0, depth), kind)

    def keep(product, slot):
        for at in range(columns // 128):
            natural[slot, at] = product[:, at * 128 : (at + 1) * 128]

    def every(slot, start, size, stride):
        return jnp.concatenate(
            [
                natural[slot, at, pl.ds(start, size, stride=stride), :]
                for at in range(columns // 128)
            ],
            axis=1,
        ).astype(jnp.bfloat16)

    with scope("w_table"):
        table_load.wait()
    base_cos = table[0, pl.ds(length + me, 1), :]
    base_sin = table[1, pl.ds(length + me, 1), :]
    inner_cos = table[0, 0:length]
    inner_sin = table[1, 0:length]
    cosine = base_cos * inner_cos - base_sin * inner_sin
    sine = base_sin * inner_cos + base_cos * inner_sin
    wide = columns // cosine.shape[1]
    cosine = jnp.concatenate([cosine] * wide, axis=1)
    sine = jnp.concatenate([sine] * wide, axis=1) * jnp.where(first_half, -1.0, 1.0)
    first_product = None
    for index in range(chunks):
        with scope(f"w_load{index}"):
            take(weights.at[7, pl.ds(0, 2 * chunk)], load_sem.at[1 + index])
        term = product_of(7, index * chunk, chunk)
        first_product = term if first_product is None else first_product + term
    for _ in range(3):
        waiting.pop(0).start()

    def far(kind):
        with scope(f"p_far{kind}"):
            keep(turned(first_product, 1) if kind == 1 else project(2, kind), kind)
            for index in range(FAR_DILATION):
                far_send[kind, index] = every(kind, index, far_steps, FAR_DILATION)
        if kind == 1:
            with scope("w_barrier"):
                pl.semaphore_wait(barrier, n - 1 + m - 1)

    def far_go(kind, index):
        for distance in range(1, n):
            target = lax.rem(me + distance, n)
            remote(
                far_send.at[kind, target * classes + index],
                far_recv.at[kind, index, me], far_sem.at[0], far_sem.at[1 + index], "sp", target,
            ).start()
        pltpu.make_async_copy(
            far_send.at[kind, me * classes + index], far_recv.at[kind, index, me],
            far_sem.at[1 + index],
        ).start()

    def middle(kind):
        with scope(f"p_mid{kind}"):
            keep(project(1, kind), 3 + kind)
            for index in range(2):
                own = every(3 + kind, 2 * side + index, steps, MIDDLE_DILATION)
                other = every(3 + kind, 2 * (1 - side) + index, steps, MIDDLE_DILATION)
                if kind == 0:
                    mid_q[index, pl.ds(side, 1)] = own[None]
                else:
                    mid_kv[kind - 1, index, pl.ds(1 + side, 1)] = own[None]
                mid_send[kind, index] = other
            landing = mid_q.at[:, side] if kind == 0 else mid_kv.at[kind - 1, :, 1 + side]
        remote(
            mid_send.at[kind], landing, pair_sem.at[0], pair_sem.at[1 if kind else 2],
            "sp", partner,
        ).start()

    lean = 2 * side - 1
    has_ahead = (me + 2 * lean >= 0) & (me + 2 * lean < n)
    has_behind = (me - 2 * lean >= 0) & (me - 2 * lean < n)
    direct = remote(
        mid_kv.at[:, :, 1 + side], mid_kv.at[:, :, 3 * (1 - side)],
        hop_sem.at[0], hop_sem.at[1], "sp", lax.rem(me + 2 * lean + n, n),
    )
    relay = remote(
        mid_kv.at[:, :, 2 - side], mid_kv.at[:, :, 3 * side],
        hop_sem.at[2], hop_sem.at[3], "sp", lax.rem(me - 2 * lean + n, n),
    )

    for kind in (1, 2, 0):
        far(kind)
        far_go(kind, 0)
    middle(1)
    middle(2)

    @pl.when(has_ahead)
    def _():
        direct.start()

    far_go(1, 1)
    far_go(2, 1)
    far_go(0, 1)
    middle(0)

    for kind in (1, 2):
        with scope(f"p_first{kind}"):
            kv_first[kind - 1, halo : halo + length] = project(0, kind).astype(jnp.bfloat16)

    first_up = remote(
        kv_first.at[:, pl.ds(length, halo)], kv_first.at[:, pl.ds(0, halo)],
        first_sem.at[0], first_sem.at[1], "sp", lax.rem(me + 1, n),
    )
    first_down = remote(
        kv_first.at[:, pl.ds(halo, halo)], kv_first.at[:, pl.ds(halo + length, halo)],
        first_sem.at[2], first_sem.at[3], "sp", lax.rem(me + n - 1, n),
    )

    @pl.when(me < n - 1)
    def _():
        first_up.start()

    @pl.when(me > 0)
    def _():
        first_down.start()

    @pl.when(me == 0)
    def _():
        kv_first[:, :halo] = jnp.zeros((2, halo, columns), jnp.bfloat16)

    @pl.when(me == n - 1)
    def _():
        kv_first[:, halo + length :] = jnp.zeros((2, halo, columns), jnp.bfloat16)

    @pl.when(me < 2)
    def _():
        mid_kv[:, :, 0] = jnp.zeros_like(mid_kv[:, :, 0])

    @pl.when(me >= n - 2)
    def _():
        mid_kv[:, :, 3] = jnp.zeros_like(mid_kv[:, :, 3])

    with scope("p_first0"):
        keep(project(0, 0), 6)
        first_queries = jnp.concatenate(
            [
                every(6, start + part, halo, 2)
                for start in range(0, length, tile)
                for part in range(2)
            ],
            axis=0,
        )

    with scope("w_pair"):
        take(mid_kv.at[:, :, 2 - side], pair_sem.at[1])

    @pl.when(has_behind)
    def _():
        relay.start()

    class_len = n * far_steps
    far_bias = band_bias(class_len, class_len, 0, 0, class_len)
    row16 = lax.broadcasted_iota(jnp.int32, (class_len, 128), 0) % far_steps
    lane16 = lax.broadcasted_iota(jnp.int32, (class_len, 128), 1)
    diagonal = lane16 % far_steps == row16

    def far_class(index):
        with scope(f"w_far{index}"):
            take(far_recv.at[:, index], far_sem.at[1 + index])
        with scope(f"c_far{index}"):
            queries, keys, values = (
                far_recv[kind, index].reshape(class_len, columns) for kind in range(3)
            )
            out, lses = attend(queries, keys, values, far_bias)
            back_send[index] = out.astype(jnp.bfloat16).reshape(n, far_steps, columns)
            spread = sum(
                jnp.where(diagonal & (lane16 // far_steps == head), lse, 0.0)
                for head, lse in enumerate(lses)
            )
            lse_send[index] = jnp.sum(spread.reshape(n, far_steps, 128), axis=1, keepdims=True)
        for which, (source, landing) in enumerate(((back_send, back_recv), (lse_send, lse_recv))):
            for peer in range(n - 1):
                target = peer + jnp.where(me <= peer, 1, 0)
                remote(
                    source.at[index, target], landing.at[index, me],
                    back_sem.at[which], back_sem.at[2 + index], "sp", target,
                ).start()
            pltpu.make_async_copy(
                source.at[index, me], landing.at[index, me], back_sem.at[2 + index]
            ).start()

    far_class(0)

    with scope("w_hop"):
        take(mid_q.at[:, 1 - side], pair_sem.at[2])

        @pl.when(has_ahead)
        def _():
            direct.wait_send()
            relay.wait_recv()

        @pl.when(has_behind)
        def _():
            relay.wait_send()
            direct.wait_recv()

    low = jnp.where(me < 2, steps, 0)
    high = jnp.where(me >= n - 2, 3 * steps, 4 * steps)
    middle_bias = band_bias(2 * steps, 4 * steps, -steps, low, high)
    sub_row = lax.broadcasted_iota(jnp.int32, (2 * steps, 128), 0) % steps // 8
    sub_lane = lax.broadcasted_iota(jnp.int32, (2 * steps, 128), 1)
    for index in range(2):
        with scope(f"c_mid{index}"):
            out, lses = attend(
                mid_q[index].reshape(2 * steps, columns),
                mid_kv[0, index].reshape(4 * steps, columns),
                mid_kv[1, index].reshape(4 * steps, columns),
                middle_bias,
            )
            mid_ret[index] = out.astype(jnp.bfloat16).reshape(2, steps, columns)
            spread = sum(
                jnp.where((sub_lane % sub == sub_row) & (sub_lane // sub == head), lse, 0.0)
                for head, lse in enumerate(lses)
            )
            mid_lse[index] = jnp.sum(spread.reshape(2, sub, 8, 128), axis=1)
        for source, landing in ((mid_ret, mid_back), (mid_lse, mid_lse_back)):
            remote(
                source.at[index, 1 - side], landing.at[index],
                ret_sem.at[0], ret_sem.at[1 + index], "sp", partner,
            ).start()

    far_class(1)

    with scope("w_first"):
        @pl.when(me < n - 1)
        def _():
            first_up.wait_send()
            first_down.wait_recv()

        @pl.when(me > 0)
        def _():
            first_down.wait_send()
            first_up.wait_recv()

    first_outs = []
    first_lses = []
    with scope("c_first"):
        for start in range(0, length, tile):
            width = tile + 2 * halo
            low = halo - start - me * length
            high = halo - start + (n - me) * length
            out, lses = attend(
                first_queries[start : start + tile],
                kv_first[0, start : start + width],
                kv_first[1, start : start + width],
                band_bias(tile, width, -halo, low, high, 2),
            )
            first_outs.append(out)
            first_lses.append(
                sum(lse * head_mask(columns, head) for head, lse in enumerate(lses))
            )

    def lane_spread(group):
        term = lax.broadcasted_iota(jnp.int32, (128, columns), 0)
        column = lax.broadcasted_iota(jnp.int32, (128, columns), 1)
        keep = (term // group == column // HEAD_DIM).astype(jnp.float32).astype(jnp.bfloat16)
        return jnp.concatenate([keep] * 3, axis=0)

    middle_spread = lane_spread(sub)
    far_spread = lane_spread(far_steps)
    middle_natural = one_hot(
        piece, lambda row: row // 2 + steps * ((row % 2 + side) % 2)
    )
    far_natural = one_hot(piece, lambda row: (row % n) * far_steps + row // n)
    position = lax.broadcasted_iota(jnp.int32, (piece, 128), 0) // n
    lane_part = lax.broadcasted_iota(jnp.int32, (piece, 128), 1)
    far_keep = (lane_part % far_steps == position) & (lane_part < heads * far_steps)
    middle_keep = (sub_lane % sub == sub_row) & (sub_lane < heads * sub)

    def near(part):
        with scope(f"w_ret{part}"):
            take(natural.at[0, 0, pl.ds(0, ret_rows)], ret_sem.at[1 + part])
        with scope(f"c_near{part}"):
            block = jnp.concatenate([mid_ret[part, side], mid_back[part]], axis=0)
            block = jnp.dot(middle_natural, block, preferred_element_type=jnp.float32)
            lse = jnp.concatenate(
                [mid_lse[part, side]] * sub + [mid_lse_back[part]] * sub, axis=0
            )
            lse = in_terms(jnp.where(middle_keep, lse, 0.0))
            lse = jnp.dot(middle_natural, lse, preferred_element_type=jnp.float32)
            middle_lse = jnp.dot(
                lse.astype(jnp.bfloat16), middle_spread, preferred_element_type=jnp.float32
            )
            rows = slice(part * halo, (part + 1) * halo)
            first_out = jnp.concatenate([out[rows] for out in first_outs], axis=0)
            first_lse = jnp.concatenate([lse[rows] for lse in first_lses], axis=0)
            top = jnp.maximum(first_lse, middle_lse)
            first_w = jnp.exp(first_lse - top)
            middle_w = jnp.exp(middle_lse - top)
        return first_w * first_out + middle_w * block, first_w + middle_w, top

    chips = m // 2
    sibling = mine + 1 - 2 * lax.rem(mine, 2)

    core = lax.rem(mine, 2)

    def rows_of(part):
        return pl.ds(part * piece, piece)

    def hand(part, source, slot, target):
        remote(
            merged_all.at[source, rows_of(part)], merged_all.at[slot, rows_of(part)],
            tp_send_sem.at[0], tp_recv_sem.at[part, slot - 1], "tp", target,
        ).start()

    def arrived(part, slot):
        take(merged_all.at[slot, rows_of(part)], tp_recv_sem.at[part, slot - 1])

    def term(part, slot, owner):
        rows = pl.ds(pl.multiple_of(lax.rem(owner + m, m) * columns, columns), columns)
        return jnp.dot(
            merged_all[slot, part * piece : (part + 1) * piece],
            out_weight[rows, :],
            preferred_element_type=jnp.float32,
        )

    totals = []
    with scope("w_outw"):
        out_load.wait()
    for part in range(2):
        total, weight, near_top = near(part)
        with scope(f"w_back{part}"):
            take(natural.at[0, 0, pl.ds(0, back_rows)], back_sem.at[2 + part])
        with scope(f"c_merge{part}"):
            far_out = jnp.dot(
                far_natural,
                back_recv[part].reshape(piece, columns),
                preferred_element_type=jnp.float32,
            )
            lse = jnp.concatenate([lse_recv[part].reshape(n, 128)] * (piece // n), axis=0)
            lse = jnp.where(far_keep, lse, 0.0)
            far_lse = jnp.dot(in_terms(lse), far_spread, preferred_element_type=jnp.float32)
            top = jnp.maximum(near_top, far_lse)
            near_w = jnp.exp(near_top - top)
            far_w = jnp.exp(far_lse - top)
            merged = (near_w * total + far_w * far_out) / (near_w * weight + far_w)
            merged_all[0, part * piece : (part + 1) * piece] = merged.astype(jnp.bfloat16)
        for chip in range(1, chips):
            hand(part, 0, chip, lax.rem(mine + 2 * chip, m))
            if part == 1:
                @pl.when(core == 0)
                def _():
                    hand(part, 0, chips + chip, lax.rem(mine + 2 * chip + 1, m))
        hand(part, 0, chips, sibling)
        totals.append(term(part, 0, mine))

    take(mid_send, pair_sem.at[0])
    take(far_send.at[:, pl.ds(0, FAR_DILATION - classes)], far_sem.at[0])
    take(back_send.at[:, pl.ds(0, n - 1)], back_sem.at[0])
    take(lse_send.at[:, pl.ds(0, n - 1)], back_sem.at[1])
    take(natural.at[0, 0, pl.ds(0, 2 * ret_rows)], ret_sem.at[0])

    for chip in range(1, chips):
        with scope("w_chip0"):
            arrived(0, chip)
        hand(0, chip, chips + chip, sibling)
    with scope("w_sib0"):
        arrived(0, chips)
    totals[0] = totals[0] + term(0, chips, sibling)
    for chip in range(1, chips):
        totals[0] = totals[0] + term(0, chip, mine - 2 * chip)
    for chip in range(1, chips):
        early = jnp.where(core == 1, chip, chips + chip)
        with scope("w_early"):
            arrived(1, early)

        @pl.when(core == 1)
        def _():
            hand(1, chip, chips + chip, sibling)

        totals[1] = totals[1] + term(1, early, mine + 1 - core - 2 * chip)
    with scope("w_sib1"):
        arrived(1, chips)
    totals[1] = totals[1] + term(1, chips, sibling)
    for chip in range(1, chips):
        with scope("w_fwd0"):
            arrived(0, chips + chip)
        totals[0] = totals[0] + term(0, chips + chip, sibling - 2 * chip)
    for chip in range(1, chips):
        late = jnp.where(core == 1, chips + chip, chip)
        with scope("w_late"):
            arrived(1, late)
        totals[1] = totals[1] + term(1, late, mine - core - 2 * chip)
    with scope("c_result"):
        for part in range(2):
            for index in range(result_wide.shape[0]):
                result_wide[index, pl.ds(part, piece, stride=2), :] = totals[part][
                    :, index * 128 : (index + 1) * 128
                ]
        for index in range(result_wide.shape[0]):
            result_ref[:, index * 128 : (index + 1) * 128] = result_wide[index].astype(
                result_ref.dtype
            )
    take(merged_all.at[pl.ds(1, m - 1)], tp_send_sem.at[0])


def turn_tables(n, length):
    half = HEAD_DIM // 2
    inverse = 1.0 / 10000.0 ** (np.arange(half, dtype=np.float32) * np.float32(2.0) / HEAD_DIM)
    inverse = np.tile(inverse.astype(np.float64), 128 // half)[None]
    positions = np.concatenate([np.arange(length), np.arange(n) * length])
    angles = positions[:, None] * inverse
    return np.stack([np.cos(angles), np.sin(angles)]).astype(np.float32)


def fused(n, m, tokens, query_weight, key_weight, value_weight, out_weight):
    length, width = tokens.shape
    columns = query_weight.shape[2]
    table = turn_tables(n, length)
    steps = length // FAR_DILATION
    span = length // MIDDLE_DILATION
    classes = FAR_DILATION // n
    bf16 = jnp.bfloat16
    hbm = pl.BlockSpec(memory_space=pl.ANY)
    vmem = pl.BlockSpec(memory_space=pltpu.VMEM)
    dma = pltpu.SemaphoreType.DMA
    return pl.pallas_call(
        functools.partial(fused_kernel, n, m),
        out_shape=pltpu.VMEM((length, out_weight.shape[1]), bf16),
        in_specs=[hbm] * 6,
        out_specs=vmem,
        scratch_shapes=[
            pltpu.VMEM((length, width), bf16),
            pltpu.VMEM((9, width, columns), bf16),
            pltpu.VMEM(out_weight.shape, bf16),
            pltpu.VMEM(table.shape, jnp.float32),
            pltpu.VMEM((2, length + 2 * SIDE_STEPS, columns), bf16),
            pltpu.VMEM((2, 2, 4, span, columns), bf16),
            pltpu.VMEM((2, 2, span, columns), bf16),
            pltpu.VMEM((3, 2, span, columns), bf16),
            pltpu.VMEM((2, 2, span, columns), bf16),
            pltpu.VMEM((2, span, columns), bf16),
            pltpu.VMEM((2, 2, 8, 128), jnp.float32),
            pltpu.VMEM((2, 8, 128), jnp.float32),
            pltpu.VMEM((3, FAR_DILATION, steps, columns), bf16),
            pltpu.VMEM((3, classes, n, steps, columns), bf16),
            pltpu.VMEM((classes, n, steps, columns), bf16),
            pltpu.VMEM((classes, n, steps, columns), bf16),
            pltpu.VMEM((classes, n, 1, 128), jnp.float32),
            pltpu.VMEM((classes, n, 1, 128), jnp.float32),
            pltpu.VMEM((m, length, columns), bf16),
            pltpu.VMEM((out_weight.shape[1] // 128, length, 128), jnp.float32),
            pltpu.VMEM((7, columns // 128, length, 128), jnp.float32),
            dma((6,)),
            dma((4,)),
            dma((3,)),
            dma((4,)),
            dma((3,)),
            dma((1 + classes,)),
            dma((2 + classes,)),
            dma((1,)),
            dma((2, m - 1)),
        ],
        compiler_params=pltpu.CompilerParams(
            collective_id=0, has_side_effects=True, vmem_limit_bytes=60 * 1024 * 1024
        ),
    )(tokens, query_weight, key_weight, value_weight, out_weight, jnp.asarray(table))


def planned(n, m, *arrays):
    length, columns = arrays[0].shape[0], arrays[1].shape[2]
    fits = (
        n == 8
        and m % 2 == 0
        and FAR_DILATION == 2 * n
        and MIDDLE_DILATION == 4
        and length == SIDE_STEPS * MIDDLE_DILATION
        and length % (FAR_DILATION * 16) == 0
        and columns % 128 == 0
        and arrays[4].shape[1] % 128 == 0
        and 3 * (columns // HEAD_DIM) <= 128
        and columns // HEAD_DIM * (length // FAR_DILATION) <= 128
    )
    if fits:
        return fused(n, m, *arrays)
    return per_device(*arrays)


def solution(mesh):
    placed = (
        P("sp", None),
        P(None, None, "tp"),
        P(None, None, "tp"),
        P(None, None, "tp"),
        P(None, "tp"),
    )
    return jax.shard_map(
        functools.partial(planned, mesh.shape["sp"], mesh.shape["tp"]),
        mesh=mesh,
        in_specs=placed,
        out_specs=P("sp", "tp"),
        check_vma=False,
    )
```

```python
import functools
import math

import jax
import numpy as np
import jax.numpy as jnp
from jax import lax
from jax.experimental import pallas as pl
from jax.experimental.pallas import tpu as pltpu
from jax.sharding import PartitionSpec as P

HEAD_DIM = 64
SIDE_STEPS = 64
MIDDLE_DILATION = 4
FAR_DILATION = 16
MESH = pl.DeviceIdType.MESH


def shifted(block, axis, distance):
    devices = range(lax.axis_size(axis))
    route = [(i - distance, i) for i in devices if i - distance in devices]
    return lax.ppermute(block, axis, route)


def with_halo(block, sides, width):
    for axis, dim in sides:
        count = lax.axis_size(axis)
        forward = [(i, i + 1) for i in range(count - 1)]
        backward = [(target, source) for source, target in forward]
        low = lax.ppermute(
            lax.slice_in_dim(block, block.shape[dim] - width, None, axis=dim), axis, forward
        )
        high = lax.ppermute(lax.slice_in_dim(block, 0, width, axis=dim), axis, backward)
        block = jnp.concatenate([low, block, high], axis=dim)
    return block


def rotate(projected, offset_pos):
    length, columns = projected.shape
    heads = columns // HEAD_DIM
    half = HEAD_DIM // 2
    positions = (offset_pos + jnp.arange(length)).astype(jnp.float32)
    inverse = 1.0 / 10000.0 ** (jnp.arange(half, dtype=jnp.float32) * 2.0 / HEAD_DIM)
    angles = positions[:, None] * inverse[None, :]
    angles = jnp.concatenate([angles, angles], axis=-1)
    cosine_table = jnp.cos(angles)[:, None, :]
    sine = jnp.sin(angles)[:, None, :]
    shaped = projected.reshape(length, heads, HEAD_DIM)
    turned = jnp.concatenate([-shaped[..., half:], shaped[..., :half]], axis=-1)
    return (shaped * cosine_table + turned * sine).reshape(length, columns)


def banded(queries, key_ext, value_ext, dilation, offset_pos, seq_len):
    length, columns = queries.shape
    heads = columns // HEAD_DIM
    class_len = length // dilation
    block_len = math.gcd(SIDE_STEPS, class_len)
    blocks = class_len // block_len
    extra = 2 * SIDE_STEPS // block_len
    query_blocks = queries.reshape(blocks, block_len, dilation, heads, HEAD_DIM)
    key_blocks = key_ext.reshape(blocks + extra, block_len, dilation, heads, HEAD_DIM)
    value_blocks = value_ext.reshape(blocks + extra, block_len, dilation, heads, HEAD_DIM)
    key_win = jnp.concatenate(
        [key_blocks[shift_idx : shift_idx + blocks] for shift_idx in range(extra + 1)], axis=1
    )
    value_win = jnp.concatenate(
        [value_blocks[shift_idx : shift_idx + blocks] for shift_idx in range(extra + 1)], axis=1
    )
    scores = jnp.einsum(
        "bqrhe,bkrhe->brhqk", query_blocks, key_win, preferred_element_type=jnp.float32
    )
    scores = scores * HEAD_DIM ** (-0.5)
    width_keys = key_win.shape[1]
    relative = jnp.arange(width_keys)[None, :] - jnp.arange(block_len)[:, None]
    within = (relative >= 0) & (relative <= 2 * SIDE_STEPS)
    key_rows = jnp.arange(blocks)[:, None] * block_len + jnp.arange(width_keys)[None, :]
    spots = (
        offset_pos
        - SIDE_STEPS * dilation
        + dilation * key_rows[:, :, None]
        + jnp.arange(dilation)[None, None, :]
    )
    inside = (spots >= 0) & (spots < seq_len)
    allowed = within[None, None, None] & jnp.transpose(inside, (0, 2, 1))[:, :, None, None, :]
    scores = jnp.where(allowed, scores, -1e30)
    row_max = jnp.max(scores, axis=-1, keepdims=True)
    expo = jnp.exp(scores - row_max)
    denom = jnp.sum(expo, axis=-1)
    probs = expo.astype(jnp.bfloat16)
    summed = jnp.einsum("brhqk,bkrhe->bqrhe", probs, value_win, preferred_element_type=jnp.float32)
    group_out = summed / jnp.transpose(denom, (0, 3, 1, 2))[..., None]
    log_sum = row_max[..., 0] + jnp.log(denom)
    log_sum = jnp.transpose(log_sum, (0, 3, 1, 2)).reshape(length, heads)
    return (group_out.reshape(length, columns), log_sum)


def collect(own_block, needed, direction):
    collected = own_block[None]
    while collected.shape[0] < needed + 1:
        stride = collected.shape[0]
        to_send = min(stride, needed + 1 - stride)
        arrived = shifted(collected[:to_send], "sp", direction * stride)
        collected = jnp.concatenate([collected, arrived], axis=0)
    return collected[1:]


def per_device(tokens, query_weight, key_weight, value_weight, out_weight):
    length = tokens.shape[0]
    offset_pos = lax.axis_index("sp") * length
    seq_len = lax.axis_size("sp") * length
    group_dilations = (1, MIDDLE_DILATION, FAR_DILATION)
    query_list = []
    pairs = []
    for group_idx in range(3):
        queries = rotate(
            jnp.dot(tokens, query_weight[group_idx], preferred_element_type=jnp.float32), offset_pos
        )
        keys_here = rotate(
            jnp.dot(tokens, key_weight[group_idx], preferred_element_type=jnp.float32), offset_pos
        )
        values_here = jnp.dot(tokens, value_weight[group_idx], preferred_element_type=jnp.float32)
        query_list.append(queries.astype(jnp.bfloat16))
        pairs.append(
            jnp.stack([keys_here.astype(jnp.bfloat16), values_here.astype(jnp.bfloat16)], axis=0)
        )
    middle_span_length = SIDE_STEPS * MIDDLE_DILATION
    first_ext = with_halo(pairs[0], (("sp", 1),), SIDE_STEPS)
    middle_ext = with_halo(pairs[1], (("sp", 1),), middle_span_length)
    far_span_length = SIDE_STEPS * FAR_DILATION
    needed = -(-far_span_length // length)
    lower_blocks = collect(pairs[2], needed, 1)
    upper_blocks = collect(pairs[2], needed, -1)
    columns = pairs[2].shape[2]
    lower_flat = jnp.moveaxis(lower_blocks[::-1], 0, 1).reshape(2, needed * length, columns)
    upper_flat = jnp.moveaxis(upper_blocks, 0, 1).reshape(2, needed * length, columns)
    far_full = jnp.concatenate([lower_flat, pairs[2], upper_flat], axis=1)
    extended = (first_ext, middle_ext, far_full)
    outputs = []
    log_sums = []
    for group_idx in range(3):
        group_out, log_sum = banded(
            query_list[group_idx],
            extended[group_idx][0],
            extended[group_idx][1],
            group_dilations[group_idx],
            offset_pos,
            seq_len,
        )
        outputs.append(group_out)
        log_sums.append(log_sum)
    merge_w = jax.nn.softmax(jnp.stack(log_sums, axis=0), axis=0)
    heads = columns // HEAD_DIM
    stacked = jnp.stack(outputs, axis=0).reshape(3, length, heads, HEAD_DIM)
    merged = (
        jnp.sum(merge_w[..., None] * stacked, axis=0).reshape(length, columns).astype(jnp.bfloat16)
    )
    mixed = jnp.dot(
        lax.all_gather(merged, "tp", axis=1, tiled=True),
        out_weight,
        preferred_element_type=jnp.float32,
    )
    return mixed.astype(jnp.bfloat16)


def remote(src, dst, send_sem, recv_sem, axis, target):
    return pltpu.make_async_remote_copy(
        src_ref=src,
        dst_ref=dst,
        send_sem=send_sem,
        recv_sem=recv_sem,
        device_id={axis: target},
        device_id_type=MESH,
    )


def head_mask(columns, head):
    lane = lax.broadcasted_iota(jnp.int32, (1, columns), 1)
    return (lane // HEAD_DIM == head).astype(jnp.float32)


def attend(queries, keys, values, bias):
    rows, columns = queries.shape
    heads = columns // HEAD_DIM
    masks = [head_mask(columns, head) for head in range(heads)]
    stacked = jnp.concatenate([queries * mask.astype(jnp.bfloat16) for mask in masks], axis=0)
    scores = lax.dot_general(
        stacked, keys, (((1,), (1,)), ((), ())), preferred_element_type=jnp.float32
    )
    width = keys.shape[0]
    scores = (scores.reshape(heads, rows, width) + bias[None]).reshape(heads * rows, width)
    row_max = jnp.max(scores, axis=-1, keepdims=True)
    expo = jnp.exp(scores - row_max)
    denom = jnp.sum(expo, axis=-1, keepdims=True)
    summed = jnp.dot(expo.astype(jnp.bfloat16), values, preferred_element_type=jnp.float32)
    summed = summed / denom
    lse = row_max + jnp.log(denom)
    parts = [slice(head * rows, (head + 1) * rows) for head in range(heads)]
    out = sum(summed[part] * mask for part, mask in zip(parts, masks))
    return out, [lse[part] for part in parts]


def in_terms(block):
    terms = []
    for _ in range(3):
        rounded = block.astype(jnp.bfloat16)
        terms.append(rounded)
        block = block - rounded.astype(jnp.float32)
    return jnp.concatenate(terms, axis=1)


def band_bias(rows, width, offset, low, high, stride=1):
    query = lax.broadcasted_iota(jnp.int32, (rows, width), 0)
    key = lax.broadcasted_iota(jnp.int32, (rows, width), 1)
    query = (query % (rows // stride)) * stride + query // (rows // stride)
    step = key + offset - query
    keep = (step >= -SIDE_STEPS) & (step <= SIDE_STEPS) & (key >= low) & (key < high)
    return jnp.where(keep, 0.0, -1e30)


def one_hot(size, source_of_row):
    row = lax.broadcasted_iota(jnp.int32, (size, size), 0)
    column = lax.broadcasted_iota(jnp.int32, (size, size), 1)
    return (source_of_row(row) == column).astype(jnp.float32).astype(jnp.bfloat16)


def scope(name):
    return jax.named_scope(name)


def take(ref, sem):
    pltpu.make_async_copy(ref, ref, sem).wait()


def fused_kernel(
    n, m, tokens_hbm, query_hbm, key_hbm, value_hbm, out_hbm, table_hbm, result_ref,
    tokens, weights, out_weight, table, kv_first, mid_kv, mid_q, mid_send, mid_ret, mid_back,
    mid_lse, mid_lse_back, far_send, far_recv, back_send, back_recv, lse_send, lse_recv,
    merged_all, result_wide, natural, load_sem, first_sem, pair_sem, hop_sem, ret_sem,
    far_sem, back_sem, tp_send_sem, tp_recv_sem,
):
    me = lax.axis_index("sp")
    mine = lax.axis_index("tp")
    side = lax.rem(me, 2)
    partner = me + 1 - 2 * side
    length, columns = tokens.shape[0], weights.shape[-1]
    depth = tokens.shape[1]
    heads = columns // HEAD_DIM
    half = HEAD_DIM // 2
    classes = FAR_DILATION // n
    far_steps = length // FAR_DILATION
    halo = SIDE_STEPS
    steps = length // MIDDLE_DILATION
    piece = length // 2
    sub = steps // 8
    back_rows = n * (far_steps * columns // 256 + 1)
    ret_rows = steps * columns // 256 + 8

    table_load = pltpu.make_async_copy(table_hbm, table, load_sem.at[0])
    chunks = 4
    chunk = depth // chunks
    for index in range(chunks):
        part = pl.ds(index * chunk, chunk)
        sem = load_sem.at[1 + index]
        pltpu.make_async_copy(tokens_hbm.at[:, part], tokens.at[:, part], sem).start()
        pltpu.make_async_copy(key_hbm.at[2, part], weights.at[7, part], sem).start()
        if index == 1:
            table_load.start()
    out_load = pltpu.make_async_copy(out_hbm, out_weight, load_sem.at[2])
    sources = (query_hbm, key_hbm, value_hbm)
    order = ((2, 2), (1, 1), (1, 2), (2, 0), (1, 0), (0, 1), (0, 2), (0, 0))
    waiting = []
    weight_loads = {}
    for index, (group, kind) in enumerate(order):
        slot = group * 3 + kind
        load = pltpu.make_async_copy(
            sources[kind].at[group], weights.at[slot], load_sem.at[(5, 1, 2, 3, 4, 0, 5, 1)[index]]
        )
        weight_loads[group, kind] = load
        waiting.append(load)
    waiting.append(out_load)
    waiting.pop(0).start()

    barrier = pltpu.get_barrier_semaphore()
    for distance in range(1, n):
        pl.semaphore_signal(
            barrier, inc=1, device_id={"sp": lax.rem(me + distance, n)}, device_id_type=MESH
        )
    for distance in range(1, m):
        pl.semaphore_signal(
            barrier, inc=1, device_id={"tp": lax.rem(mine + distance, m)}, device_id_type=MESH
        )

    tile = 2 * halo
    lane = lax.broadcasted_iota(jnp.int32, (1, columns), 1)
    first_half = lane % HEAD_DIM < half

    def product_of(slot, low, size):
        return jnp.dot(
            tokens[:, low : low + size],
            weights[slot, low : low + size],
            preferred_element_type=jnp.float32,
        )

    def rolled(block, shift):
        return jnp.concatenate(
            [pltpu.roll(block[:, at : at + 128], shift, 1) for at in range(0, columns, 128)], axis=1
        )

    def turned(product, kind):
        if kind < 2:
            later = rolled(product, 128 - half)
            earlier = rolled(product, half)
            product = product * cosine + jnp.where(first_half, later, earlier) * sine
        if kind == 0:
            product = product * HEAD_DIM ** (-0.5)
        return product

    def project(group, kind):
        slot = group * 3 + kind
        weight_loads[group, kind].wait()
        if waiting:
            waiting.pop(0).start()
        return turned(product_of(slot, 0, depth), kind)

    def keep(product, slot):
        for at in range(columns // 128):
            natural[slot, at] = product[:, at * 128 : (at + 1) * 128]

    def every(slot, start, size, stride):
        return jnp.concatenate(
            [
                natural[slot, at, pl.ds(start, size, stride=stride), :]
                for at in range(columns // 128)
            ],
            axis=1,
        ).astype(jnp.bfloat16)

    first_product = None
    for index in range(chunks):
        with scope(f"w_load{index}"):
            take(weights.at[7, pl.ds(0, 2 * chunk)], load_sem.at[1 + index])
        term = product_of(7, index * chunk, chunk)
        first_product = term if first_product is None else first_product + term
    with scope("w_table"):
        table_load.wait()
    base_cos = table[0, pl.ds(length + me, 1), :]
    base_sin = table[1, pl.ds(length + me, 1), :]
    inner_cos = table[0, 0:length]
    inner_sin = table[1, 0:length]
    cosine = base_cos * inner_cos - base_sin * inner_sin
    sine = base_sin * inner_cos + base_cos * inner_sin
    wide = columns // cosine.shape[1]
    cosine = jnp.concatenate([cosine] * wide, axis=1)
    sine = jnp.concatenate([sine] * wide, axis=1) * jnp.where(first_half, -1.0, 1.0)
    for _ in range(3):
        waiting.pop(0).start()

    def far_pick(kind, parity):
        for index in range(parity, FAR_DILATION, classes):
            far_send[kind, index] = every(kind, index, far_steps, FAR_DILATION)

    def far(kind):
        with scope(f"p_far{kind}"):
            keep(turned(first_product, 1) if kind == 1 else project(2, kind), kind)
            far_pick(kind, 0)
        if kind == 1:
            with scope("w_barrier"):
                pl.semaphore_wait(barrier, n - 1 + m - 1)

    def far_go(kind, index):
        for distance in range(1, n):
            target = lax.rem(me + distance, n)
            remote(
                far_send.at[kind, target * classes + index],
                far_recv.at[kind, index, me], far_sem.at[0], far_sem.at[1 + index], "sp", target,
            ).start()
        pltpu.make_async_copy(
            far_send.at[kind, me * classes + index], far_recv.at[kind, index, me],
            far_sem.at[1 + index],
        ).start()

    def middle(kind):
        with scope(f"p_mid{kind}"):
            keep(project(1, kind), 3 + kind)
            for index in range(2):
                own = every(3 + kind, 2 * side + index, steps, MIDDLE_DILATION)
                other = every(3 + kind, 2 * (1 - side) + index, steps, MIDDLE_DILATION)
                if kind == 0:
                    mid_q[index, pl.ds(side, 1)] = own[None]
                else:
                    mid_kv[kind - 1, index, pl.ds(1 + side, 1)] = own[None]
                mid_send[kind, index] = other
            landing = mid_q.at[:, side] if kind == 0 else mid_kv.at[kind - 1, :, 1 + side]
        remote(
            mid_send.at[kind], landing, pair_sem.at[0], pair_sem.at[1 if kind else 2],
            "sp", partner,
        ).start()

    lean = 2 * side - 1
    has_ahead = (me + 2 * lean >= 0) & (me + 2 * lean < n)
    has_behind = (me - 2 * lean >= 0) & (me - 2 * lean < n)
    direct = remote(
        mid_kv.at[:, :, 1 + side], mid_kv.at[:, :, 3 * (1 - side)],
        hop_sem.at[0], hop_sem.at[1], "sp", lax.rem(me + 2 * lean + n, n),
    )
    relay = remote(
        mid_kv.at[:, :, 2 - side], mid_kv.at[:, :, 3 * side],
        hop_sem.at[2], hop_sem.at[3], "sp", lax.rem(me - 2 * lean + n, n),
    )

    far(1)
    far_go(1, 0)
    far(2)
    far_go(2, 0)
    middle(1)
    middle(2)

    @pl.when(has_ahead)
    def _():
        direct.start()

    far(0)
    far_go(0, 0)
    for kind in (1, 2, 0):
        far_pick(kind, 1)
        far_go(kind, 1)
    middle(0)

    for kind in (1, 2):
        with scope(f"p_first{kind}"):
            kv_first[kind - 1, halo : halo + length] = project(0, kind).astype(jnp.bfloat16)

    first_up = remote(
        kv_first.at[:, pl.ds(length, halo)], kv_first.at[:, pl.ds(0, halo)],
        first_sem.at[0], first_sem.at[1], "sp", lax.rem(me + 1, n),
    )
    first_down = remote(
        kv_first.at[:, pl.ds(halo, halo)], kv_first.at[:, pl.ds(halo + length, halo)],
        first_sem.at[2], first_sem.at[3], "sp", lax.rem(me + n - 1, n),
    )

    @pl.when(me < n - 1)
    def _():
        first_up.start()

    @pl.when(me > 0)
    def _():
        first_down.start()

    @pl.when(me == 0)
    def _():
        kv_first[:, :halo] = jnp.zeros((2, halo, columns), jnp.bfloat16)

    @pl.when(me == n - 1)
    def _():
        kv_first[:, halo + length :] = jnp.zeros((2, halo, columns), jnp.bfloat16)

    @pl.when(me < 2)
    def _():
        mid_kv[:, :, 0] = jnp.zeros_like(mid_kv[:, :, 0])

    @pl.when(me >= n - 2)
    def _():
        mid_kv[:, :, 3] = jnp.zeros_like(mid_kv[:, :, 3])

    with scope("p_first0"):
        keep(project(0, 0), 6)
        first_queries = jnp.concatenate(
            [
                every(6, start + part, halo, 2)
                for start in range(0, length, tile)
                for part in range(2)
            ],
            axis=0,
        )

    with scope("w_pair"):
        take(mid_kv.at[:, :, 2 - side], pair_sem.at[1])

    @pl.when(has_behind)
    def _():
        relay.start()

    class_len = n * far_steps
    far_bias = band_bias(class_len, class_len, 0, 0, class_len)
    row16 = lax.broadcasted_iota(jnp.int32, (class_len, 128), 0) % far_steps
    lane16 = lax.broadcasted_iota(jnp.int32, (class_len, 128), 1)
    diagonal = lane16 % far_steps == row16

    def far_class(index):
        with scope(f"w_far{index}"):
            take(far_recv.at[:, index], far_sem.at[1 + index])
        with scope(f"c_far{index}"):
            queries, keys, values = (
                far_recv[kind, index].reshape(class_len, columns) for kind in range(3)
            )
            out, lses = attend(queries, keys, values, far_bias)
            back_send[index] = out.astype(jnp.bfloat16).reshape(n, far_steps, columns)
            spread = sum(
                jnp.where(diagonal & (lane16 // far_steps == head), lse, 0.0)
                for head, lse in enumerate(lses)
            )
            lse_send[index] = jnp.sum(spread.reshape(n, far_steps, 128), axis=1, keepdims=True)
        for which, (source, landing) in enumerate(((back_send, back_recv), (lse_send, lse_recv))):
            for peer in range(n - 1):
                target = peer + jnp.where(me <= peer, 1, 0)
                remote(
                    source.at[index, target], landing.at[index, me],
                    back_sem.at[which], back_sem.at[2 + index], "sp", target,
                ).start()
            pltpu.make_async_copy(
                source.at[index, me], landing.at[index, me], back_sem.at[2 + index]
            ).start()

    far_class(0)

    with scope("w_hop"):
        take(mid_q.at[:, 1 - side], pair_sem.at[2])

        @pl.when(has_ahead)
        def _():
            direct.wait_send()
            relay.wait_recv()

        @pl.when(has_behind)
        def _():
            relay.wait_send()
            direct.wait_recv()

    low = jnp.where(me < 2, steps, 0)
    high = jnp.where(me >= n - 2, 3 * steps, 4 * steps)
    middle_bias = band_bias(2 * steps, 4 * steps, -steps, low, high)
    sub_row = lax.broadcasted_iota(jnp.int32, (2 * steps, 128), 0) % steps // 8
    sub_lane = lax.broadcasted_iota(jnp.int32, (2 * steps, 128), 1)
    def middle_class(index):
        with scope(f"c_mid{index}"):
            out, lses = attend(
                mid_q[index].reshape(2 * steps, columns),
                mid_kv[0, index].reshape(4 * steps, columns),
                mid_kv[1, index].reshape(4 * steps, columns),
                middle_bias,
            )
            mid_ret[index] = out.astype(jnp.bfloat16).reshape(2, steps, columns)
            spread = sum(
                jnp.where((sub_lane % sub == sub_row) & (sub_lane // sub == head), lse, 0.0)
                for head, lse in enumerate(lses)
            )
            mid_lse[index] = jnp.sum(spread.reshape(2, sub, 8, 128), axis=1)
        for source, landing in ((mid_ret, mid_back), (mid_lse, mid_lse_back)):
            remote(
                source.at[index, 1 - side], landing.at[index],
                ret_sem.at[0], ret_sem.at[1 + index], "sp", partner,
            ).start()

    middle_class(0)
    far_class(1)
    middle_class(1)

    with scope("w_first"):
        @pl.when(me < n - 1)
        def _():
            first_up.wait_send()
            first_down.wait_recv()

        @pl.when(me > 0)
        def _():
            first_down.wait_send()
            first_up.wait_recv()

    first_outs = []
    first_lses = []
    with scope("c_first"):
        for start in range(0, length, tile):
            width = tile + 2 * halo
            low = halo - start - me * length
            high = halo - start + (n - me) * length
            out, lses = attend(
                first_queries[start : start + tile],
                kv_first[0, start : start + width],
                kv_first[1, start : start + width],
                band_bias(tile, width, -halo, low, high, 2),
            )
            first_outs.append(out)
            first_lses.append(
                sum(lse * head_mask(columns, head) for head, lse in enumerate(lses))
            )

    def lane_spread(group):
        term = lax.broadcasted_iota(jnp.int32, (128, columns), 0)
        column = lax.broadcasted_iota(jnp.int32, (128, columns), 1)
        keep = (term // group == column // HEAD_DIM).astype(jnp.float32).astype(jnp.bfloat16)
        return jnp.concatenate([keep] * 3, axis=0)

    middle_spread = lane_spread(sub)
    far_spread = lane_spread(far_steps)
    middle_natural = one_hot(
        piece, lambda row: row // 2 + steps * ((row % 2 + side) % 2)
    )
    far_natural = one_hot(piece, lambda row: (row % n) * far_steps + row // n)
    position = lax.broadcasted_iota(jnp.int32, (piece, 128), 0) // n
    lane_part = lax.broadcasted_iota(jnp.int32, (piece, 128), 1)
    far_keep = (lane_part % far_steps == position) & (lane_part < heads * far_steps)
    middle_keep = (sub_lane % sub == sub_row) & (sub_lane < heads * sub)

    def near(part):
        with scope(f"w_ret{part}"):
            take(natural.at[0, 0, pl.ds(0, ret_rows)], ret_sem.at[1 + part])
        with scope(f"c_near{part}"):
            block = jnp.concatenate([mid_ret[part, side], mid_back[part]], axis=0)
            block = jnp.dot(middle_natural, block, preferred_element_type=jnp.float32)
            lse = jnp.concatenate(
                [mid_lse[part, side]] * sub + [mid_lse_back[part]] * sub, axis=0
            )
            lse = in_terms(jnp.where(middle_keep, lse, 0.0))
            lse = jnp.dot(middle_natural, lse, preferred_element_type=jnp.float32)
            middle_lse = jnp.dot(
                lse.astype(jnp.bfloat16), middle_spread, preferred_element_type=jnp.float32
            )
            rows = slice(part * halo, (part + 1) * halo)
            first_out = jnp.concatenate([out[rows] for out in first_outs], axis=0)
            first_lse = jnp.concatenate([lse[rows] for lse in first_lses], axis=0)
            top = jnp.maximum(first_lse, middle_lse)
            first_w = jnp.exp(first_lse - top)
            middle_w = jnp.exp(middle_lse - top)
        return first_w * first_out + middle_w * block, first_w + middle_w, top

    chips = m // 2
    sibling = mine + 1 - 2 * lax.rem(mine, 2)

    core = lax.rem(mine, 2)

    def rows_of(part):
        return pl.ds(part * piece, piece)

    def hand(part, source, slot, target):
        remote(
            merged_all.at[source, rows_of(part)], merged_all.at[slot, rows_of(part)],
            tp_send_sem.at[0], tp_recv_sem.at[part, slot - 1], "tp", target,
        ).start()

    def arrived(part, slot):
        take(merged_all.at[slot, rows_of(part)], tp_recv_sem.at[part, slot - 1])

    def term(part, slot, owner):
        rows = pl.ds(pl.multiple_of(lax.rem(owner + m, m) * columns, columns), columns)
        return jnp.dot(
            merged_all[slot, part * piece : (part + 1) * piece],
            out_weight[rows, :],
            preferred_element_type=jnp.float32,
        )

    totals = []
    with scope("w_outw"):
        out_load.wait()
    for part in range(2):
        total, weight, near_top = near(part)
        with scope(f"w_back{part}"):
            take(natural.at[0, 0, pl.ds(0, back_rows)], back_sem.at[2 + part])
        with scope(f"c_merge{part}"):
            far_out = jnp.dot(
                far_natural,
                back_recv[part].reshape(piece, columns),
                preferred_element_type=jnp.float32,
            )
            lse = jnp.concatenate([lse_recv[part].reshape(n, 128)] * (piece // n), axis=0)
            lse = jnp.where(far_keep, lse, 0.0)
            far_lse = jnp.dot(in_terms(lse), far_spread, preferred_element_type=jnp.float32)
            top = jnp.maximum(near_top, far_lse)
            near_w = jnp.exp(near_top - top)
            far_w = jnp.exp(far_lse - top)
            merged = (near_w * total + far_w * far_out) / (near_w * weight + far_w)
            merged_all[0, part * piece : (part + 1) * piece] = merged.astype(jnp.bfloat16)
        hand(part, 0, chips, sibling)
        for chip in range(1, chips):
            hand(part, 0, chip, lax.rem(mine + 2 * chip, m))
            if part == 1:
                @pl.when(core == 0)
                def _():
                    hand(part, 0, chips + chip, lax.rem(mine + 2 * chip + 1, m))
        totals.append(term(part, 0, mine))

    take(mid_send, pair_sem.at[0])
    take(far_send.at[:, pl.ds(0, FAR_DILATION - classes)], far_sem.at[0])
    take(back_send.at[:, pl.ds(0, n - 1)], back_sem.at[0])
    take(lse_send.at[:, pl.ds(0, n - 1)], back_sem.at[1])
    take(natural.at[0, 0, pl.ds(0, 2 * ret_rows)], ret_sem.at[0])

    for chip in range(1, chips):
        with scope("w_chip0"):
            arrived(0, chip)
        hand(0, chip, chips + chip, sibling)
    with scope("w_sib0"):
        arrived(0, chips)
    totals[0] = totals[0] + term(0, chips, sibling)
    for chip in range(1, chips):
        totals[0] = totals[0] + term(0, chip, mine - 2 * chip)
    for chip in range(1, chips):
        early = jnp.where(core == 1, chip, chips + chip)
        with scope("w_early"):
            arrived(1, early)

        @pl.when(core == 1)
        def _():
            hand(1, chip, chips + chip, sibling)

        totals[1] = totals[1] + term(1, early, mine + 1 - core - 2 * chip)
    with scope("w_sib1"):
        arrived(1, chips)
    totals[1] = totals[1] + term(1, chips, sibling)
    for chip in range(1, chips):
        with scope("w_fwd0"):
            arrived(0, chips + chip)
        totals[0] = totals[0] + term(0, chips + chip, sibling - 2 * chip)
    for chip in range(1, chips):
        late = jnp.where(core == 1, chips + chip, chip)
        with scope("w_late"):
            arrived(1, late)
        totals[1] = totals[1] + term(1, late, mine - core - 2 * chip)
    with scope("c_result"):
        for part in range(2):
            for index in range(result_wide.shape[0]):
                result_wide[index, pl.ds(part, piece, stride=2), :] = totals[part][
                    :, index * 128 : (index + 1) * 128
                ]
        for index in range(result_wide.shape[0]):
            result_ref[:, index * 128 : (index + 1) * 128] = result_wide[index].astype(
                result_ref.dtype
            )
    take(merged_all.at[pl.ds(1, m - 1)], tp_send_sem.at[0])


def turn_tables(n, length):
    half = HEAD_DIM // 2
    inverse = 1.0 / 10000.0 ** (np.arange(half, dtype=np.float32) * np.float32(2.0) / HEAD_DIM)
    inverse = np.tile(inverse.astype(np.float64), 128 // half)[None]
    positions = np.concatenate([np.arange(length), np.arange(n) * length])
    angles = positions[:, None] * inverse
    return np.stack([np.cos(angles), np.sin(angles)]).astype(np.float32)


def fused(n, m, tokens, query_weight, key_weight, value_weight, out_weight):
    length, width = tokens.shape
    columns = query_weight.shape[2]
    table = turn_tables(n, length)
    steps = length // FAR_DILATION
    span = length // MIDDLE_DILATION
    classes = FAR_DILATION // n
    bf16 = jnp.bfloat16
    hbm = pl.BlockSpec(memory_space=pl.ANY)
    vmem = pl.BlockSpec(memory_space=pltpu.VMEM)
    dma = pltpu.SemaphoreType.DMA
    return pl.pallas_call(
        functools.partial(fused_kernel, n, m),
        out_shape=pltpu.VMEM((length, out_weight.shape[1]), bf16),
        in_specs=[hbm] * 6,
        out_specs=vmem,
        scratch_shapes=[
            pltpu.VMEM((length, width), bf16),
            pltpu.VMEM((9, width, columns), bf16),
            pltpu.VMEM(out_weight.shape, bf16),
            pltpu.VMEM(table.shape, jnp.float32),
            pltpu.VMEM((2, length + 2 * SIDE_STEPS, columns), bf16),
            pltpu.VMEM((2, 2, 4, span, columns), bf16),
            pltpu.VMEM((2, 2, span, columns), bf16),
            pltpu.VMEM((3, 2, span, columns), bf16),
            pltpu.VMEM((2, 2, span, columns), bf16),
            pltpu.VMEM((2, span, columns), bf16),
            pltpu.VMEM((2, 2, 8, 128), jnp.float32),
            pltpu.VMEM((2, 8, 128), jnp.float32),
            pltpu.VMEM((3, FAR_DILATION, steps, columns), bf16),
            pltpu.VMEM((3, classes, n, steps, columns), bf16),
            pltpu.VMEM((classes, n, steps, columns), bf16),
            pltpu.VMEM((classes, n, steps, columns), bf16),
            pltpu.VMEM((classes, n, 1, 128), jnp.float32),
            pltpu.VMEM((classes, n, 1, 128), jnp.float32),
            pltpu.VMEM((m, length, columns), bf16),
            pltpu.VMEM((out_weight.shape[1] // 128, length, 128), jnp.float32),
            pltpu.VMEM((7, columns // 128, length, 128), jnp.float32),
            dma((6,)),
            dma((4,)),
            dma((3,)),
            dma((4,)),
            dma((3,)),
            dma((1 + classes,)),
            dma((2 + classes,)),
            dma((1,)),
            dma((2, m - 1)),
        ],
        compiler_params=pltpu.CompilerParams(
            collective_id=0, has_side_effects=True, vmem_limit_bytes=60 * 1024 * 1024
        ),
    )(tokens, query_weight, key_weight, value_weight, out_weight, jnp.asarray(table))


def planned(n, m, *arrays):
    length, columns = arrays[0].shape[0], arrays[1].shape[2]
    fits = (
        n == 8
        and m % 2 == 0
        and FAR_DILATION == 2 * n
        and MIDDLE_DILATION == 4
        and length == SIDE_STEPS * MIDDLE_DILATION
        and length % (FAR_DILATION * 16) == 0
        and columns % 128 == 0
        and arrays[4].shape[1] % 128 == 0
        and 3 * (columns // HEAD_DIM) <= 128
        and columns // HEAD_DIM * (length // FAR_DILATION) <= 128
    )
    if fits:
        return fused(n, m, *arrays)
    return per_device(*arrays)


def solution(mesh):
    placed = (
        P("sp", None),
        P(None, None, "tp"),
        P(None, None, "tp"),
        P(None, None, "tp"),
        P(None, "tp"),
    )
    return jax.shard_map(
        functools.partial(planned, mesh.shape["sp"], mesh.shape["tp"]),
        mesh=mesh,
        in_specs=placed,
        out_specs=P("sp", "tp"),
        check_vma=False,
    )
```

```python
import functools
import math

import jax
import numpy as np
import jax.numpy as jnp
from jax import lax
from jax.experimental import pallas as pl
from jax.experimental.pallas import tpu as pltpu
from jax.sharding import PartitionSpec as P

HEAD_DIM = 64
SIDE_STEPS = 64
MIDDLE_DILATION = 4
FAR_DILATION = 16
MESH = pl.DeviceIdType.MESH


def shifted(block, axis, distance):
    devices = range(lax.axis_size(axis))
    route = [(i - distance, i) for i in devices if i - distance in devices]
    return lax.ppermute(block, axis, route)


def with_halo(block, sides, width):
    for axis, dim in sides:
        count = lax.axis_size(axis)
        forward = [(i, i + 1) for i in range(count - 1)]
        backward = [(target, source) for source, target in forward]
        low = lax.ppermute(
            lax.slice_in_dim(block, block.shape[dim] - width, None, axis=dim), axis, forward
        )
        high = lax.ppermute(lax.slice_in_dim(block, 0, width, axis=dim), axis, backward)
        block = jnp.concatenate([low, block, high], axis=dim)
    return block


def rotate(projected, offset_pos):
    length, columns = projected.shape
    heads = columns // HEAD_DIM
    half = HEAD_DIM // 2
    positions = (offset_pos + jnp.arange(length)).astype(jnp.float32)
    inverse = 1.0 / 10000.0 ** (jnp.arange(half, dtype=jnp.float32) * 2.0 / HEAD_DIM)
    angles = positions[:, None] * inverse[None, :]
    angles = jnp.concatenate([angles, angles], axis=-1)
    cosine_table = jnp.cos(angles)[:, None, :]
    sine = jnp.sin(angles)[:, None, :]
    shaped = projected.reshape(length, heads, HEAD_DIM)
    turned = jnp.concatenate([-shaped[..., half:], shaped[..., :half]], axis=-1)
    return (shaped * cosine_table + turned * sine).reshape(length, columns)


def banded(queries, key_ext, value_ext, dilation, offset_pos, seq_len):
    length, columns = queries.shape
    heads = columns // HEAD_DIM
    class_len = length // dilation
    block_len = math.gcd(SIDE_STEPS, class_len)
    blocks = class_len // block_len
    extra = 2 * SIDE_STEPS // block_len
    query_blocks = queries.reshape(blocks, block_len, dilation, heads, HEAD_DIM)
    key_blocks = key_ext.reshape(blocks + extra, block_len, dilation, heads, HEAD_DIM)
    value_blocks = value_ext.reshape(blocks + extra, block_len, dilation, heads, HEAD_DIM)
    key_win = jnp.concatenate(
        [key_blocks[shift_idx : shift_idx + blocks] for shift_idx in range(extra + 1)], axis=1
    )
    value_win = jnp.concatenate(
        [value_blocks[shift_idx : shift_idx + blocks] for shift_idx in range(extra + 1)], axis=1
    )
    scores = jnp.einsum(
        "bqrhe,bkrhe->brhqk", query_blocks, key_win, preferred_element_type=jnp.float32
    )
    scores = scores * HEAD_DIM ** (-0.5)
    width_keys = key_win.shape[1]
    relative = jnp.arange(width_keys)[None, :] - jnp.arange(block_len)[:, None]
    within = (relative >= 0) & (relative <= 2 * SIDE_STEPS)
    key_rows = jnp.arange(blocks)[:, None] * block_len + jnp.arange(width_keys)[None, :]
    spots = (
        offset_pos
        - SIDE_STEPS * dilation
        + dilation * key_rows[:, :, None]
        + jnp.arange(dilation)[None, None, :]
    )
    inside = (spots >= 0) & (spots < seq_len)
    allowed = within[None, None, None] & jnp.transpose(inside, (0, 2, 1))[:, :, None, None, :]
    scores = jnp.where(allowed, scores, -1e30)
    row_max = jnp.max(scores, axis=-1, keepdims=True)
    expo = jnp.exp(scores - row_max)
    denom = jnp.sum(expo, axis=-1)
    probs = expo.astype(jnp.bfloat16)
    summed = jnp.einsum("brhqk,bkrhe->bqrhe", probs, value_win, preferred_element_type=jnp.float32)
    group_out = summed / jnp.transpose(denom, (0, 3, 1, 2))[..., None]
    log_sum = row_max[..., 0] + jnp.log(denom)
    log_sum = jnp.transpose(log_sum, (0, 3, 1, 2)).reshape(length, heads)
    return (group_out.reshape(length, columns), log_sum)


def collect(own_block, needed, direction):
    collected = own_block[None]
    while collected.shape[0] < needed + 1:
        stride = collected.shape[0]
        to_send = min(stride, needed + 1 - stride)
        arrived = shifted(collected[:to_send], "sp", direction * stride)
        collected = jnp.concatenate([collected, arrived], axis=0)
    return collected[1:]


def per_device(tokens, query_weight, key_weight, value_weight, out_weight):
    length = tokens.shape[0]
    offset_pos = lax.axis_index("sp") * length
    seq_len = lax.axis_size("sp") * length
    group_dilations = (1, MIDDLE_DILATION, FAR_DILATION)
    query_list = []
    pairs = []
    for group_idx in range(3):
        queries = rotate(
            jnp.dot(tokens, query_weight[group_idx], preferred_element_type=jnp.float32), offset_pos
        )
        keys_here = rotate(
            jnp.dot(tokens, key_weight[group_idx], preferred_element_type=jnp.float32), offset_pos
        )
        values_here = jnp.dot(tokens, value_weight[group_idx], preferred_element_type=jnp.float32)
        query_list.append(queries.astype(jnp.bfloat16))
        pairs.append(
            jnp.stack([keys_here.astype(jnp.bfloat16), values_here.astype(jnp.bfloat16)], axis=0)
        )
    middle_span_length = SIDE_STEPS * MIDDLE_DILATION
    first_ext = with_halo(pairs[0], (("sp", 1),), SIDE_STEPS)
    middle_ext = with_halo(pairs[1], (("sp", 1),), middle_span_length)
    far_span_length = SIDE_STEPS * FAR_DILATION
    needed = -(-far_span_length // length)
    lower_blocks = collect(pairs[2], needed, 1)
    upper_blocks = collect(pairs[2], needed, -1)
    columns = pairs[2].shape[2]
    lower_flat = jnp.moveaxis(lower_blocks[::-1], 0, 1).reshape(2, needed * length, columns)
    upper_flat = jnp.moveaxis(upper_blocks, 0, 1).reshape(2, needed * length, columns)
    far_full = jnp.concatenate([lower_flat, pairs[2], upper_flat], axis=1)
    extended = (first_ext, middle_ext, far_full)
    outputs = []
    log_sums = []
    for group_idx in range(3):
        group_out, log_sum = banded(
            query_list[group_idx],
            extended[group_idx][0],
            extended[group_idx][1],
            group_dilations[group_idx],
            offset_pos,
            seq_len,
        )
        outputs.append(group_out)
        log_sums.append(log_sum)
    merge_w = jax.nn.softmax(jnp.stack(log_sums, axis=0), axis=0)
    heads = columns // HEAD_DIM
    stacked = jnp.stack(outputs, axis=0).reshape(3, length, heads, HEAD_DIM)
    merged = (
        jnp.sum(merge_w[..., None] * stacked, axis=0).reshape(length, columns).astype(jnp.bfloat16)
    )
    mixed = jnp.dot(
        lax.all_gather(merged, "tp", axis=1, tiled=True),
        out_weight,
        preferred_element_type=jnp.float32,
    )
    return mixed.astype(jnp.bfloat16)


def remote(src, dst, send_sem, recv_sem, axis, target):
    return pltpu.make_async_remote_copy(
        src_ref=src,
        dst_ref=dst,
        send_sem=send_sem,
        recv_sem=recv_sem,
        device_id={axis: target},
        device_id_type=MESH,
    )


def head_mask(columns, head):
    lane = lax.broadcasted_iota(jnp.int32, (1, columns), 1)
    return (lane // HEAD_DIM == head).astype(jnp.float32)


def attend(queries, keys, values, bias):
    rows, columns = queries.shape
    heads = columns // HEAD_DIM
    masks = [head_mask(columns, head) for head in range(heads)]
    stacked = jnp.concatenate([queries * mask.astype(jnp.bfloat16) for mask in masks], axis=0)
    scores = lax.dot_general(
        stacked, keys, (((1,), (1,)), ((), ())), preferred_element_type=jnp.float32
    )
    width = keys.shape[0]
    scores = (scores.reshape(heads, rows, width) + bias[None]).reshape(heads * rows, width)
    row_max = jnp.max(scores, axis=-1, keepdims=True)
    expo = jnp.exp(scores - row_max)
    denom = jnp.sum(expo, axis=-1, keepdims=True)
    summed = jnp.dot(expo.astype(jnp.bfloat16), values, preferred_element_type=jnp.float32)
    summed = summed / denom
    lse = row_max + jnp.log(denom)
    parts = [slice(head * rows, (head + 1) * rows) for head in range(heads)]
    out = sum(summed[part] * mask for part, mask in zip(parts, masks))
    return out, [lse[part] for part in parts]


def in_terms(block):
    terms = []
    for _ in range(3):
        rounded = block.astype(jnp.bfloat16)
        terms.append(rounded)
        block = block - rounded.astype(jnp.float32)
    return jnp.concatenate(terms, axis=1)


def band_bias(rows, width, offset, low, high, stride=1):
    query = lax.broadcasted_iota(jnp.int32, (rows, width), 0)
    key = lax.broadcasted_iota(jnp.int32, (rows, width), 1)
    query = (query % (rows // stride)) * stride + query // (rows // stride)
    step = key + offset - query
    keep = (step >= -SIDE_STEPS) & (step <= SIDE_STEPS) & (key >= low) & (key < high)
    return jnp.where(keep, 0.0, -1e30)


def one_hot(size, source_of_row):
    row = lax.broadcasted_iota(jnp.int32, (size, size), 0)
    column = lax.broadcasted_iota(jnp.int32, (size, size), 1)
    return (source_of_row(row) == column).astype(jnp.float32).astype(jnp.bfloat16)


def scope(name):
    return jax.named_scope(name)


def take(ref, sem):
    pltpu.make_async_copy(ref, ref, sem).wait()


def fused_kernel(
    n, m, tokens_hbm, query_hbm, key_hbm, value_hbm, out_hbm, table_hbm, result_ref,
    tokens, weights, out_weight, table, kv_first, mid_kv, mid_q, mid_send, mid_ret, mid_back,
    mid_lse, mid_lse_back, far_send, far_recv, back_send, back_recv, lse_send, lse_recv,
    merged_all, result_wide, natural, load_sem, first_sem, pair_sem, hop_sem, ret_sem,
    far_sem, back_sem, tp_send_sem, tp_recv_sem,
):
    me = lax.axis_index("sp")
    mine = lax.axis_index("tp")
    side = lax.rem(me, 2)
    partner = me + 1 - 2 * side
    length, columns = tokens.shape[0], weights.shape[-1]
    depth = tokens.shape[1]
    heads = columns // HEAD_DIM
    half = HEAD_DIM // 2
    classes = FAR_DILATION // n
    far_steps = length // FAR_DILATION
    halo = SIDE_STEPS
    steps = length // MIDDLE_DILATION
    piece = length // 2
    sub = steps // 8
    back_rows = n * (far_steps * columns // 256 + 1)
    ret_rows = steps * columns // 256 + 8

    table_load = pltpu.make_async_copy(table_hbm, table, load_sem.at[0])
    chunks = 4
    chunk = depth // chunks
    for index in range(chunks):
        part = pl.ds(index * chunk, chunk)
        sem = load_sem.at[1 + index]
        pltpu.make_async_copy(tokens_hbm.at[:, part], tokens.at[:, part], sem).start()
        pltpu.make_async_copy(key_hbm.at[2, part], weights.at[7, part], sem).start()
        if index == 1:
            table_load.start()
    out_load = pltpu.make_async_copy(out_hbm, out_weight, load_sem.at[2])
    sources = (query_hbm, key_hbm, value_hbm)
    order = ((2, 2), (1, 1), (1, 2), (2, 0), (1, 0), (0, 1), (0, 2), (0, 0))
    waiting = []
    weight_loads = {}
    for index, (group, kind) in enumerate(order):
        slot = group * 3 + kind
        load = pltpu.make_async_copy(
            sources[kind].at[group], weights.at[slot], load_sem.at[(5, 1, 2, 3, 4, 0, 5, 1)[index]]
        )
        weight_loads[group, kind] = load
        waiting.append(load)
    waiting.append(out_load)
    waiting.pop(0).start()

    barrier = pltpu.get_barrier_semaphore()
    for distance in range(1, n):
        pl.semaphore_signal(
            barrier, inc=1, device_id={"sp": lax.rem(me + distance, n)}, device_id_type=MESH
        )
    for distance in range(1, m):
        pl.semaphore_signal(
            barrier, inc=1, device_id={"tp": lax.rem(mine + distance, m)}, device_id_type=MESH
        )

    tile = 2 * halo
    lane = lax.broadcasted_iota(jnp.int32, (1, columns), 1)
    first_half = lane % HEAD_DIM < half

    def product_of(slot, low, size):
        return jnp.dot(
            tokens[:, low : low + size],
            weights[slot, low : low + size],
            preferred_element_type=jnp.float32,
        )

    def rolled(block, shift):
        return jnp.concatenate(
            [pltpu.roll(block[:, at : at + 128], shift, 1) for at in range(0, columns, 128)], axis=1
        )

    def turned(product, kind):
        if kind < 2:
            later = rolled(product, 128 - half)
            earlier = rolled(product, half)
            product = product * cosine + jnp.where(first_half, later, earlier) * sine
        if kind == 0:
            product = product * HEAD_DIM ** (-0.5)
        return product

    def project(group, kind):
        slot = group * 3 + kind
        weight_loads[group, kind].wait()
        if waiting:
            waiting.pop(0).start()
        return turned(product_of(slot, 0, depth), kind)

    def keep(product, slot):
        for at in range(columns // 128):
            natural[slot, at] = product[:, at * 128 : (at + 1) * 128]

    def every(slot, start, size, stride):
        return jnp.concatenate(
            [
                natural[slot, at, pl.ds(start, size, stride=stride), :]
                for at in range(columns // 128)
            ],
            axis=1,
        ).astype(jnp.bfloat16)

    first_product = None
    for index in range(chunks):
        with scope(f"w_load{index}"):
            take(weights.at[7, pl.ds(0, 2 * chunk)], load_sem.at[1 + index])
        term = product_of(7, index * chunk, chunk)
        first_product = term if first_product is None else first_product + term
    with scope("w_table"):
        table_load.wait()
    base_cos = table[0, pl.ds(length + me, 1), :]
    base_sin = table[1, pl.ds(length + me, 1), :]
    inner_cos = table[0, 0:length]
    inner_sin = table[1, 0:length]
    cosine = base_cos * inner_cos - base_sin * inner_sin
    sine = base_sin * inner_cos + base_cos * inner_sin
    wide = columns // cosine.shape[1]
    cosine = jnp.concatenate([cosine] * wide, axis=1)
    sine = jnp.concatenate([sine] * wide, axis=1) * jnp.where(first_half, -1.0, 1.0)
    for _ in range(3):
        waiting.pop(0).start()

    def far_pick(kind, parity):
        for index in range(parity, FAR_DILATION, classes):
            far_send[kind, index] = every(kind, index, far_steps, FAR_DILATION)

    def far(kind):
        with scope(f"p_far{kind}"):
            keep(turned(first_product, 1) if kind == 1 else project(2, kind), kind)
            far_pick(kind, 0)
        if kind == 1:
            with scope("w_barrier"):
                pl.semaphore_wait(barrier, n - 1 + m - 1)

    def far_go(kind, index):
        for distance in range(1, n):
            target = lax.rem(me + distance, n)
            remote(
                far_send.at[kind, target * classes + index],
                far_recv.at[kind, index, me], far_sem.at[0], far_sem.at[1 + index], "sp", target,
            ).start()
        pltpu.make_async_copy(
            far_send.at[kind, me * classes + index], far_recv.at[kind, index, me],
            far_sem.at[1 + index],
        ).start()

    def middle(kind):
        with scope(f"p_mid{kind}"):
            keep(project(1, kind), 3 + kind)
            for index in range(2):
                own = every(3 + kind, 2 * side + index, steps, MIDDLE_DILATION)
                other = every(3 + kind, 2 * (1 - side) + index, steps, MIDDLE_DILATION)
                if kind == 0:
                    mid_q[index, pl.ds(side, 1)] = own[None]
                else:
                    mid_kv[kind - 1, index, pl.ds(1 + side, 1)] = own[None]
                mid_send[kind, index] = other
            landing = mid_q.at[:, side] if kind == 0 else mid_kv.at[kind - 1, :, 1 + side]
        remote(
            mid_send.at[kind], landing, pair_sem.at[0], pair_sem.at[1 if kind else 2],
            "sp", partner,
        ).start()

    lean = 2 * side - 1
    has_ahead = (me + 2 * lean >= 0) & (me + 2 * lean < n)
    has_behind = (me - 2 * lean >= 0) & (me - 2 * lean < n)
    direct = remote(
        mid_kv.at[:, :, 1 + side], mid_kv.at[:, :, 3 * (1 - side)],
        hop_sem.at[0], hop_sem.at[1], "sp", lax.rem(me + 2 * lean + n, n),
    )
    relay = remote(
        mid_kv.at[:, :, 2 - side], mid_kv.at[:, :, 3 * side],
        hop_sem.at[2], hop_sem.at[3], "sp", lax.rem(me - 2 * lean + n, n),
    )

    far(1)
    far_go(1, 0)
    far(2)
    far_go(2, 0)

    @pl.when(me >= n // 2)
    def _():
        for kind in (1, 2):
            far_pick(kind, 1)
            far_go(kind, 1)

    middle(1)
    middle(2)

    @pl.when(has_ahead)
    def _():
        direct.start()

    far(0)
    far_go(0, 0)
    @pl.when(me < n // 2)
    def _():
        for kind in (1, 2):
            far_pick(kind, 1)
            far_go(kind, 1)

    far_pick(0, 1)
    far_go(0, 1)
    middle(0)

    for kind in (1, 2):
        with scope(f"p_first{kind}"):
            kv_first[kind - 1, halo : halo + length] = project(0, kind).astype(jnp.bfloat16)

    first_up = remote(
        kv_first.at[:, pl.ds(length, halo)], kv_first.at[:, pl.ds(0, halo)],
        first_sem.at[0], first_sem.at[1], "sp", lax.rem(me + 1, n),
    )
    first_down = remote(
        kv_first.at[:, pl.ds(halo, halo)], kv_first.at[:, pl.ds(halo + length, halo)],
        first_sem.at[2], first_sem.at[3], "sp", lax.rem(me + n - 1, n),
    )

    @pl.when(me < n - 1)
    def _():
        first_up.start()

    @pl.when(me > 0)
    def _():
        first_down.start()

    @pl.when(me == 0)
    def _():
        kv_first[:, :halo] = jnp.zeros((2, halo, columns), jnp.bfloat16)

    @pl.when(me == n - 1)
    def _():
        kv_first[:, halo + length :] = jnp.zeros((2, halo, columns), jnp.bfloat16)

    @pl.when(me < 2)
    def _():
        mid_kv[:, :, 0] = jnp.zeros_like(mid_kv[:, :, 0])

    @pl.when(me >= n - 2)
    def _():
        mid_kv[:, :, 3] = jnp.zeros_like(mid_kv[:, :, 3])

    with scope("p_first0"):
        keep(project(0, 0), 6)
        first_queries = jnp.concatenate(
            [
                every(6, start + part, halo, 2)
                for start in range(0, length, tile)
                for part in range(2)
            ],
            axis=0,
        )

    with scope("w_pair"):
        take(mid_kv.at[:, :, 2 - side], pair_sem.at[1])

    @pl.when(has_behind)
    def _():
        relay.start()

    class_len = n * far_steps
    far_bias = band_bias(class_len, class_len, 0, 0, class_len)
    row16 = lax.broadcasted_iota(jnp.int32, (class_len, 128), 0) % far_steps
    lane16 = lax.broadcasted_iota(jnp.int32, (class_len, 128), 1)
    diagonal = lane16 % far_steps == row16

    def far_class(index):
        with scope(f"w_far{index}"):
            take(far_recv.at[:, index], far_sem.at[1 + index])
        with scope(f"c_far{index}"):
            queries, keys, values = (
                far_recv[kind, index].reshape(class_len, columns) for kind in range(3)
            )
            out, lses = attend(queries, keys, values, far_bias)
            back_send[index] = out.astype(jnp.bfloat16).reshape(n, far_steps, columns)
            spread = sum(
                jnp.where(diagonal & (lane16 // far_steps == head), lse, 0.0)
                for head, lse in enumerate(lses)
            )
            lse_send[index] = jnp.sum(spread.reshape(n, far_steps, 128), axis=1, keepdims=True)
        for which, (source, landing) in enumerate(((back_send, back_recv), (lse_send, lse_recv))):
            for peer in range(n - 1):
                target = peer + jnp.where(me <= peer, 1, 0)
                remote(
                    source.at[index, target], landing.at[index, me],
                    back_sem.at[which], back_sem.at[2 + index], "sp", target,
                ).start()
            pltpu.make_async_copy(
                source.at[index, me], landing.at[index, me], back_sem.at[2 + index]
            ).start()

    far_class(0)

    @pl.when(me >= 2)
    def _():
        far_class(1)

    with scope("w_hop"):
        take(mid_q.at[:, 1 - side], pair_sem.at[2])

        @pl.when(has_ahead)
        def _():
            direct.wait_send()
            relay.wait_recv()

        @pl.when(has_behind)
        def _():
            relay.wait_send()
            direct.wait_recv()

    low = jnp.where(me < 2, steps, 0)
    high = jnp.where(me >= n - 2, 3 * steps, 4 * steps)
    middle_bias = band_bias(2 * steps, 4 * steps, -steps, low, high)
    sub_row = lax.broadcasted_iota(jnp.int32, (2 * steps, 128), 0) % steps // 8
    sub_lane = lax.broadcasted_iota(jnp.int32, (2 * steps, 128), 1)
    def middle_class(index):
        with scope(f"c_mid{index}"):
            out, lses = attend(
                mid_q[index].reshape(2 * steps, columns),
                mid_kv[0, index].reshape(4 * steps, columns),
                mid_kv[1, index].reshape(4 * steps, columns),
                middle_bias,
            )
            mid_ret[index] = out.astype(jnp.bfloat16).reshape(2, steps, columns)
            spread = sum(
                jnp.where((sub_lane % sub == sub_row) & (sub_lane // sub == head), lse, 0.0)
                for head, lse in enumerate(lses)
            )
            mid_lse[index] = jnp.sum(spread.reshape(2, sub, 8, 128), axis=1)
        for source, landing in ((mid_ret, mid_back), (mid_lse, mid_lse_back)):
            remote(
                source.at[index, 1 - side], landing.at[index],
                ret_sem.at[0], ret_sem.at[1 + index], "sp", partner,
            ).start()

    middle_class(0)
    middle_class(1)

    @pl.when(me < 2)
    def _():
        far_class(1)


    with scope("w_first"):
        @pl.when(me < n - 1)
        def _():
            first_up.wait_send()
            first_down.wait_recv()

        @pl.when(me > 0)
        def _():
            first_down.wait_send()
            first_up.wait_recv()

    first_outs = []
    first_lses = []
    with scope("c_first"):
        for start in range(0, length, tile):
            width = tile + 2 * halo
            low = halo - start - me * length
            high = halo - start + (n - me) * length
            out, lses = attend(
                first_queries[start : start + tile],
                kv_first[0, start : start + width],
                kv_first[1, start : start + width],
                band_bias(tile, width, -halo, low, high, 2),
            )
            first_outs.append(out)
            first_lses.append(
                sum(lse * head_mask(columns, head) for head, lse in enumerate(lses))
            )

    def lane_spread(group):
        term = lax.broadcasted_iota(jnp.int32, (128, columns), 0)
        column = lax.broadcasted_iota(jnp.int32, (128, columns), 1)
        keep = (term // group == column // HEAD_DIM).astype(jnp.float32).astype(jnp.bfloat16)
        return jnp.concatenate([keep] * 3, axis=0)

    middle_spread = lane_spread(sub)
    far_spread = lane_spread(far_steps)
    middle_natural = one_hot(
        piece, lambda row: row // 2 + steps * ((row % 2 + side) % 2)
    )
    far_natural = one_hot(piece, lambda row: (row % n) * far_steps + row // n)
    position = lax.broadcasted_iota(jnp.int32, (piece, 128), 0) // n
    lane_part = lax.broadcasted_iota(jnp.int32, (piece, 128), 1)
    far_keep = (lane_part % far_steps == position) & (lane_part < heads * far_steps)
    middle_keep = (sub_lane % sub == sub_row) & (sub_lane < heads * sub)

    def near(part):
        with scope(f"w_ret{part}"):
            take(natural.at[0, 0, pl.ds(0, ret_rows)], ret_sem.at[1 + part])
        with scope(f"c_near{part}"):
            block = jnp.concatenate([mid_ret[part, side], mid_back[part]], axis=0)
            block = jnp.dot(middle_natural, block, preferred_element_type=jnp.float32)
            lse = jnp.concatenate(
                [mid_lse[part, side]] * sub + [mid_lse_back[part]] * sub, axis=0
            )
            lse = in_terms(jnp.where(middle_keep, lse, 0.0))
            lse = jnp.dot(middle_natural, lse, preferred_element_type=jnp.float32)
            middle_lse = jnp.dot(
                lse.astype(jnp.bfloat16), middle_spread, preferred_element_type=jnp.float32
            )
            rows = slice(part * halo, (part + 1) * halo)
            first_out = jnp.concatenate([out[rows] for out in first_outs], axis=0)
            first_lse = jnp.concatenate([lse[rows] for lse in first_lses], axis=0)
            top = jnp.maximum(first_lse, middle_lse)
            first_w = jnp.exp(first_lse - top)
            middle_w = jnp.exp(middle_lse - top)
        return first_w * first_out + middle_w * block, first_w + middle_w, top

    chips = m // 2
    sibling = mine + 1 - 2 * lax.rem(mine, 2)

    core = lax.rem(mine, 2)

    def rows_of(part):
        return pl.ds(part * piece, piece)

    def hand(part, source, slot, target):
        remote(
            merged_all.at[source, rows_of(part)], merged_all.at[slot, rows_of(part)],
            tp_send_sem.at[0], tp_recv_sem.at[part, slot - 1], "tp", target,
        ).start()

    def arrived(part, slot):
        take(merged_all.at[slot, rows_of(part)], tp_recv_sem.at[part, slot - 1])

    def term(part, slot, owner):
        rows = pl.ds(pl.multiple_of(lax.rem(owner + m, m) * columns, columns), columns)
        return jnp.dot(
            merged_all[slot, part * piece : (part + 1) * piece],
            out_weight[rows, :],
            preferred_element_type=jnp.float32,
        )

    totals = []
    with scope("w_outw"):
        out_load.wait()
    for part in range(2):
        total, weight, near_top = near(part)
        with scope(f"w_back{part}"):
            take(natural.at[0, 0, pl.ds(0, back_rows)], back_sem.at[2 + part])
        with scope(f"c_merge{part}"):
            far_out = jnp.dot(
                far_natural,
                back_recv[part].reshape(piece, columns),
                preferred_element_type=jnp.float32,
            )
            lse = jnp.concatenate([lse_recv[part].reshape(n, 128)] * (piece // n), axis=0)
            lse = jnp.where(far_keep, lse, 0.0)
            far_lse = jnp.dot(in_terms(lse), far_spread, preferred_element_type=jnp.float32)
            top = jnp.maximum(near_top, far_lse)
            near_w = jnp.exp(near_top - top)
            far_w = jnp.exp(far_lse - top)
            merged = (near_w * total + far_w * far_out) / (near_w * weight + far_w)
            merged_all[0, part * piece : (part + 1) * piece] = merged.astype(jnp.bfloat16)
        hand(part, 0, chips, sibling)
        for chip in range(1, chips):
            hand(part, 0, chip, lax.rem(mine + 2 * chip, m))
            if part == 1:
                @pl.when(core == 0)
                def _():
                    hand(part, 0, chips + chip, lax.rem(mine + 2 * chip + 1, m))
        totals.append(term(part, 0, mine))

    take(mid_send, pair_sem.at[0])
    take(far_send.at[:, pl.ds(0, FAR_DILATION - classes)], far_sem.at[0])
    take(back_send.at[:, pl.ds(0, n - 1)], back_sem.at[0])
    take(lse_send.at[:, pl.ds(0, n - 1)], back_sem.at[1])
    take(natural.at[0, 0, pl.ds(0, 2 * ret_rows)], ret_sem.at[0])

    for chip in range(1, chips):
        with scope("w_chip0"):
            arrived(0, chip)
        hand(0, chip, chips + chip, sibling)
    with scope("w_sib0"):
        arrived(0, chips)
    totals[0] = totals[0] + term(0, chips, sibling)
    for chip in range(1, chips):
        totals[0] = totals[0] + term(0, chip, mine - 2 * chip)
    for chip in range(1, chips):
        early = jnp.where(core == 1, chip, chips + chip)
        with scope("w_early"):
            arrived(1, early)

        @pl.when(core == 1)
        def _():
            hand(1, chip, chips + chip, sibling)

        totals[1] = totals[1] + term(1, early, mine + 1 - core - 2 * chip)
    with scope("w_sib1"):
        arrived(1, chips)
    totals[1] = totals[1] + term(1, chips, sibling)
    for chip in range(1, chips):
        with scope("w_fwd0"):
            arrived(0, chips + chip)
        totals[0] = totals[0] + term(0, chips + chip, sibling - 2 * chip)
    for chip in range(1, chips):
        late = jnp.where(core == 1, chips + chip, chip)
        with scope("w_late"):
            arrived(1, late)
        totals[1] = totals[1] + term(1, late, mine - core - 2 * chip)
    with scope("c_result"):
        for part in range(2):
            for index in range(result_wide.shape[0]):
                result_wide[index, pl.ds(part, piece, stride=2), :] = totals[part][
                    :, index * 128 : (index + 1) * 128
                ]
        for index in range(result_wide.shape[0]):
            result_ref[:, index * 128 : (index + 1) * 128] = result_wide[index].astype(
                result_ref.dtype
            )
    take(merged_all.at[pl.ds(1, m - 1)], tp_send_sem.at[0])


def turn_tables(n, length):
    half = HEAD_DIM // 2
    inverse = 1.0 / 10000.0 ** (np.arange(half, dtype=np.float32) * np.float32(2.0) / HEAD_DIM)
    inverse = np.tile(inverse.astype(np.float64), 128 // half)[None]
    positions = np.concatenate([np.arange(length), np.arange(n) * length])
    angles = positions[:, None] * inverse
    return np.stack([np.cos(angles), np.sin(angles)]).astype(np.float32)


def fused(n, m, tokens, query_weight, key_weight, value_weight, out_weight):
    length, width = tokens.shape
    columns = query_weight.shape[2]
    table = turn_tables(n, length)
    steps = length // FAR_DILATION
    span = length // MIDDLE_DILATION
    classes = FAR_DILATION // n
    bf16 = jnp.bfloat16
    hbm = pl.BlockSpec(memory_space=pl.ANY)
    vmem = pl.BlockSpec(memory_space=pltpu.VMEM)
    dma = pltpu.SemaphoreType.DMA
    return pl.pallas_call(
        functools.partial(fused_kernel, n, m),
        out_shape=pltpu.VMEM((length, out_weight.shape[1]), bf16),
        in_specs=[hbm] * 6,
        out_specs=vmem,
        scratch_shapes=[
            pltpu.VMEM((length, width), bf16),
            pltpu.VMEM((9, width, columns), bf16),
            pltpu.VMEM(out_weight.shape, bf16),
            pltpu.VMEM(table.shape, jnp.float32),
            pltpu.VMEM((2, length + 2 * SIDE_STEPS, columns), bf16),
            pltpu.VMEM((2, 2, 4, span, columns), bf16),
            pltpu.VMEM((2, 2, span, columns), bf16),
            pltpu.VMEM((3, 2, span, columns), bf16),
            pltpu.VMEM((2, 2, span, columns), bf16),
            pltpu.VMEM((2, span, columns), bf16),
            pltpu.VMEM((2, 2, 8, 128), jnp.float32),
            pltpu.VMEM((2, 8, 128), jnp.float32),
            pltpu.VMEM((3, FAR_DILATION, steps, columns), bf16),
            pltpu.VMEM((3, classes, n, steps, columns), bf16),
            pltpu.VMEM((classes, n, steps, columns), bf16),
            pltpu.VMEM((classes, n, steps, columns), bf16),
            pltpu.VMEM((classes, n, 1, 128), jnp.float32),
            pltpu.VMEM((classes, n, 1, 128), jnp.float32),
            pltpu.VMEM((m, length, columns), bf16),
            pltpu.VMEM((out_weight.shape[1] // 128, length, 128), jnp.float32),
            pltpu.VMEM((7, columns // 128, length, 128), jnp.float32),
            dma((6,)),
            dma((4,)),
            dma((3,)),
            dma((4,)),
            dma((3,)),
            dma((1 + classes,)),
            dma((2 + classes,)),
            dma((1,)),
            dma((2, m - 1)),
        ],
        compiler_params=pltpu.CompilerParams(
            collective_id=0, has_side_effects=True, vmem_limit_bytes=60 * 1024 * 1024
        ),
    )(tokens, query_weight, key_weight, value_weight, out_weight, jnp.asarray(table))


def planned(n, m, *arrays):
    length, columns = arrays[0].shape[0], arrays[1].shape[2]
    fits = (
        n == 8
        and m % 2 == 0
        and FAR_DILATION == 2 * n
        and MIDDLE_DILATION == 4
        and length == SIDE_STEPS * MIDDLE_DILATION
        and length % (FAR_DILATION * 16) == 0
        and columns % 128 == 0
        and arrays[4].shape[1] % 128 == 0
        and 3 * (columns // HEAD_DIM) <= 128
        and columns // HEAD_DIM * (length // FAR_DILATION) <= 128
    )
    if fits:
        return fused(n, m, *arrays)
    return per_device(*arrays)


def solution(mesh):
    placed = (
        P("sp", None),
        P(None, None, "tp"),
        P(None, None, "tp"),
        P(None, None, "tp"),
        P(None, "tp"),
    )
    return jax.shard_map(
        functools.partial(planned, mesh.shape["sp"], mesh.shape["tp"]),
        mesh=mesh,
        in_specs=placed,
        out_specs=P("sp", "tp"),
        check_vma=False,
    )
```
